32 devices in a mesh: ep: 8 (over z, x), tp: 4 (over y, core).
Axes of the slice: x: 2, y: 2, z: 4, core: 2. Of those that a mesh axis runs over, the one named last changes fastest.
Arguments:
- tokens: bfloat16 [1024, 2048], P('ep'), may hold values from -6 to 6
- cotangent: bfloat16 [1024, 2048], P('ep'), may hold values from -1.5 to 1.5
- routes: int32 [1024, 2], P('ep'), may hold values from 0 to 3, all different within a row; in each aligned block of 128 rows (0 to 127, 128 to 255, ...) at most 96 rows name the same one
- router: bfloat16 [2048, 4], replicated, may hold values from -0.125 to 0.125
- w_gate: bfloat16 [8, 2048, 2048], P('ep', None, 'tp'), may hold values from -0.125 to 0.125
- w_up: bfloat16 [8, 2048, 2048], P('ep', None, 'tp'), may hold values from -0.125 to 0.125
- w_down: bfloat16 [8, 2048, 2048], P('ep', 'tp'), may hold values from -0.09375 to 0.09375
Outputs:
- token_grad: bfloat16 [1024, 2048], P('ep', 'tp')
- gate_grad: float32 [1024, 2], P('ep')
- grad_gate: bfloat16 [8, 2048, 2048], P('ep', None, 'tp')
- grad_up: bfloat16 [8, 2048, 2048], P('ep', None, 'tp')
- grad_down: bfloat16 [8, 2048, 2048], P('ep', 'tp')
- router_grad: float32 [2048, 4], P(('ep', 'tp'))
The draws below stay inside these ranges and needn't reach their ends.
Inputs may be any that keep to these rules, and one draw needn't show every extreme that they name: `routes`: each row names 2 different experts. In the rows of one index of ep (aligned blocks of 128 rows) no expert is named by more than 96 rows, a bound that some block reaches.
All inputs are finite; a program needn't handle non-finite values.
Results may differ from the reference program's by a relative error of at most 0.018.
Values may be sent and summed in bfloat16 or wider, within the bound.
A program may use at most 64 MiB of HBM per device.

```python
import math
import jax
import jax.numpy as jnp
import numpy as np
from jax import lax

D = 2048
FF = 4096
TOP = 2
BLOCKS = 2
TOK_EP = 128
EXPERTS = 4
TOKENS = 1024
CAP = 96
N_EP = 8
N_TP = 4


def spiked(values, key, source, target, parts, factor):
    owner, partner = [(jnp.arange(values.shape[axis_at]) // (values.shape[axis_at] // parts)).reshape([-1 if axis == axis_at else 1 for axis in range(values.ndim)]) for axis_at in (source, target)]
    chosen = jax.random.permutation(key, parts)[partner]
    strong = (owner == chosen) | (owner == (partner + parts // 2) % parts)
    return jnp.where(strong, factor * values, values)


def block_levels(stream_key, dims, pieces, least, top_value):
    def one(dim, blocks):
        steps = jax.random.uniform(jax.random.fold_in(jax.random.fold_in(stream_key, 6), dim), (blocks,), jnp.float32, least / len(pieces), top_value / len(pieces))
        return jnp.repeat(jnp.exp(steps), dims[dim] // blocks).reshape((-1,) + (1,) * (len(dims) - dim - 1))

    level = one(*pieces[0])
    for cut in pieces[1:]:
        level = level * one(*cut)
    return level


def routed_block(key, own, number, rows, number_of, top, limit, slope):
    sequence = jax.random.permutation(key, number_of)
    heavy_load, ordinary = load_shares(number_of, rows * top, limit, slope, True), load_shares(number_of, rows * top, limit, slope, False)
    places = jnp.arange(number_of)

    def named(sizes, turn):
        used = int((sizes > 0).sum())
        fixed = max(1, used // 4)
        shifted = fixed + (places - fixed + turn * (used - fixed)) % max(1, number_of - fixed)
        return jnp.zeros((number_of,), jnp.int32).at[sequence[jnp.where(places < fixed, places, shifted)]].set(jnp.asarray(sizes, jnp.int32))

    sizes = jnp.where(number % 4 == 0, named(heavy_load, number // 4), named(ordinary, number - number // 4 - 1))
    mixed = jax.random.permutation(jax.random.fold_in(own, 3), number_of)
    giver, taker = mixed[0:number_of // 2 * 2:2], mixed[1:number_of // 2 * 2:2]
    slack = jnp.minimum(sizes[giver] - 1, limit - sizes[taker]) // 2
    slack = jnp.where((giver == sequence[0]) | (taker == sequence[0]) | (sizes[taker] == 0), 0, jnp.maximum(slack, 0))
    shifted = jax.random.randint(jax.random.fold_in(own, 4), (number_of // 2,), 0, 1 << 20) % (slack + 1)
    sizes = sizes.at[giver].add(-shifted).at[taker].add(shifted)
    members = jnp.searchsorted(jnp.cumsum(sizes), jnp.arange(rows * top), side="right").astype(jnp.int32)
    table = members.reshape(top, rows).T
    table = table[jax.random.permutation(jax.random.fold_in(own, 1), rows)]
    turn = jax.random.randint(jax.random.fold_in(own, 2), (rows, 1), 0, top)
    return jnp.take_along_axis(table, (jnp.arange(top)[None, :] + turn) % top, axis=1)


def load_shares(number_of, total, most, lean, full):
    loads = [(1 << 20) // math.isqrt(standing ** lean) + 1 for standing in range(1, number_of + 1)]
    largest = most if full else min(most, max(-(-total // number_of), total * loads[0] // sum(loads)))
    least = 1 if total - largest >= number_of - 1 else 0
    holding, spare = [largest] + [least] * (number_of - 1), total - largest - least * (number_of - 1)
    while spare > 0:
        candidates = [i for i in range(1, number_of) if holding[i] < largest] or [i for i in range(1, number_of) if holding[i] < most]
        pool, left = sum([loads[i] for i in candidates]), spare
        for i in candidates:
            addition = min(most - holding[i], max(1, left * loads[i] // pool), spare)
            holding[i] = holding[i] + addition
            spare = spare - addition
    return np.array(holding)


def scatter_about(own_key, extent, spread, most, split=(), kind=jnp.bfloat16):
    drawn = spread * jax.random.normal(own_key, extent, jnp.float32)
    if split:
        drawn = drawn * block_levels(own_key, extent, split, -0.22, 0.18)
    return jnp.clip(drawn, -most, most).astype(kind)


def heavy_noise(rng, shape, deviation, bound, split, heavy, kind=jnp.bfloat16):
    entries = deviation * jax.random.normal(rng, shape, jnp.float32)
    if split:
        entries = entries * block_levels(rng, shape, split, -0.22, 0.18)
    return jnp.clip(spiked(entries, jax.random.fold_in(rng, 3), *heavy), -bound, bound).astype(kind)


def setup_inputs(seed: int = 0) -> dict:
    seeds = jax.random.split(jax.random.key(seed), 8)
    tokens = heavy_noise(seeds[0], (TOKENS, D), 1.0, 6.0, ((0, 8),), (0, 1, 8, 2.0))
    cotangent = scatter_about(seeds[1], (TOKENS, D), 0.25, 1.5, ((0, 8),))
    routes_keys = jax.random.split(jax.random.fold_in(seeds[2], 1), TOKENS // TOK_EP)
    routes_turns = jax.random.permutation(jax.random.fold_in(seeds[2], 3), TOKENS // TOK_EP)
    routes = jax.vmap(lambda own, number: routed_block(jax.random.fold_in(seeds[2], 2), own, number, TOK_EP, EXPERTS, TOP, CAP, 2))(routes_keys, routes_turns).reshape((TOKENS, TOP))
    router = scatter_about(seeds[3], (D, EXPERTS), D ** -0.5, 0.125)
    w_gate = scatter_about(seeds[4], (EXPERTS * BLOCKS, D, FF // BLOCKS), D ** -0.5, 0.125, ((0, 8), (2, 4)))
    w_up = scatter_about(seeds[5], (EXPERTS * BLOCKS, D, FF // BLOCKS), D ** -0.5, 0.125, ((0, 8), (2, 4)))
    w_down = scatter_about(seeds[6], (EXPERTS * BLOCKS, FF // BLOCKS, D), FF ** -0.5, 0.09375, ((0, 8), (1, 4)))
    return {"tokens": tokens, "cotangent": cotangent, "routes": routes, "router": router, "w_gate": w_gate, "w_up": w_up, "w_down": w_down}


def build_slots(block_routes, experts, capacity):
    flat_routes = block_routes.reshape(-1)
    labels = jnp.arange(experts, dtype=jnp.int32)
    hit_mask = (flat_routes[None, :] == labels[:, None]).astype(jnp.int32)
    rank_in = jnp.cumsum(hit_mask, axis=1, dtype=jnp.int32) - 1
    slot_ids = jnp.arange(capacity, dtype=jnp.int32)
    assigned = (hit_mask[:, None, :] == 1) & (rank_in[:, None, :] == slot_ids[None, :, None])
    return assigned.astype(jnp.float32)


def gate_pair(tokens, routes, router, experts):
    logits = jnp.dot(tokens, router, preferred_element_type=jnp.float32)
    labels = jnp.arange(experts, dtype=jnp.int32)
    picked = (routes[:, :, None] == labels[None, None, :]).astype(jnp.float32)
    chosen = jnp.sum(picked * logits[:, None, :], axis=2)
    margin = chosen[:, 0] - chosen[:, 1]
    weights = jnp.stack([jax.nn.sigmoid(margin), jax.nn.sigmoid(-margin)], axis=1)
    return picked, weights


def logit_grads(picked, weights, gate_grad):
    lead_grad = weights[:, 0] * weights[:, 1] * (gate_grad[:, 0] - gate_grad[:, 1])
    pair_grad = jnp.stack([lead_grad, -lead_grad], axis=1)
    return jnp.sum(picked * pair_grad[:, :, None], axis=1)


def expert_grads(rows_in, cot_in, gate_in, gate_weight, up_weight, down_weight):
    pre_gate = jnp.dot(rows_in, gate_weight, preferred_element_type=jnp.float32)
    pre_up = jnp.dot(rows_in, up_weight, preferred_element_type=jnp.float32)
    back_grad = lax.dot_general(cot_in, down_weight, (((1,), (1,)), ((), ())), preferred_element_type=jnp.float32)
    sig_gate = jax.nn.sigmoid(pre_gate)
    active = pre_gate * sig_gate
    hidden = (active * pre_up).astype(jnp.bfloat16)
    gate_terms = jnp.sum(hidden.astype(jnp.float32) * back_grad, axis=1)
    gate_col = gate_in.astype(jnp.float32)[:, None]
    scaled_back = gate_col * back_grad
    d_gate = (scaled_back * pre_up * sig_gate * (1.0 + pre_gate * (1.0 - sig_gate))).astype(jnp.bfloat16)
    d_up = (scaled_back * active).astype(jnp.bfloat16)
    scaled_cot = (gate_col * cot_in.astype(jnp.float32)).astype(jnp.bfloat16)
    contract_rows = (((0,), (0,)), ((), ()))
    grad_gate = lax.dot_general(rows_in, d_gate, contract_rows, preferred_element_type=jnp.float32).astype(jnp.bfloat16)
    grad_up = lax.dot_general(rows_in, d_up, contract_rows, preferred_element_type=jnp.float32).astype(jnp.bfloat16)
    grad_down = lax.dot_general(hidden, scaled_cot, contract_rows, preferred_element_type=jnp.float32).astype(jnp.bfloat16)
    return d_gate, d_up, gate_terms, grad_gate, grad_up, grad_down


def reference(tokens, cotangent, routes, router, w_gate, w_up, w_down):
    highest = lax.Precision.HIGHEST
    picked, weights = gate_pair(tokens, routes, router, EXPERTS)
    gate_send = lax.optimization_barrier(weights.astype(jnp.bfloat16)).astype(jnp.float32)
    assigned = jax.vmap(lambda block_routes: build_slots(block_routes, EXPERTS, CAP))(routes.reshape(N_EP, TOK_EP, TOP))
    by_expert = jnp.transpose(assigned, (1, 0, 2, 3))
    tok_src = tokens.reshape(N_EP, TOK_EP, D).astype(jnp.float32)
    cot_src = cotangent.reshape(N_EP, TOK_EP, D).astype(jnp.float32)
    gate_src = gate_send.reshape(N_EP, TOK_EP * TOP)
    half_ff = FF // BLOCKS
    gate_full = jnp.transpose(w_gate.reshape(EXPERTS, BLOCKS, D, half_ff), (0, 2, 1, 3)).reshape(EXPERTS, D, FF)
    up_full = jnp.transpose(w_up.reshape(EXPERTS, BLOCKS, D, half_ff), (0, 2, 1, 3)).reshape(EXPERTS, D, FF)
    down_full = w_down.reshape(EXPERTS, FF, D)
    nblocks = BLOCKS * N_TP
    block_width = FF // nblocks

    def one_expert(carry, inputs):
        dx_acc, gate_acc = carry
        slots_here, gate_weight, up_weight, down_weight = inputs
        per_token = jnp.sum(slots_here.reshape(N_EP, CAP, TOK_EP, TOP), axis=3)
        rows_in = jnp.einsum('sct,std->scd', per_token, tok_src, precision=highest).astype(jnp.bfloat16).reshape(-1, D)
        cot_in = jnp.einsum('sct,std->scd', per_token, cot_src, precision=highest).astype(jnp.bfloat16).reshape(-1, D)
        gate_in = jnp.einsum('scj,sj->sc', slots_here, gate_src, precision=highest).astype(jnp.bfloat16).reshape(-1)
        d_gate, d_up, gate_terms, grad_gate, grad_up, grad_down = expert_grads(rows_in, cot_in, gate_in, gate_weight, up_weight, down_weight)
        blocks_gate = jnp.einsum('rbh,dbh->rbd', d_gate.astype(jnp.float32).reshape(-1, nblocks, block_width),
                                 gate_weight.astype(jnp.float32).reshape(D, nblocks, block_width))
        blocks_up = jnp.einsum('rbh,dbh->rbd', d_up.astype(jnp.float32).reshape(-1, nblocks, block_width),
                               up_weight.astype(jnp.float32).reshape(D, nblocks, block_width))
        block_dx = lax.optimization_barrier((blocks_gate + blocks_up).astype(jnp.bfloat16)).astype(jnp.float32)
        pair_dx = jnp.sum(block_dx, axis=1).reshape(N_EP, CAP, D)
        dx_acc = dx_acc + jnp.einsum('sct,scd->std', per_token, pair_dx, precision=highest)
        gate_acc = gate_acc + jnp.einsum('scj,sc->sj', slots_here, gate_terms.reshape(N_EP, CAP), precision=highest)
        return (dx_acc, gate_acc), (grad_gate, grad_up, grad_down)

    start_carry = (jnp.zeros((N_EP, TOK_EP, D), jnp.float32), jnp.zeros((N_EP, TOK_EP * TOP), jnp.float32))
    (dx_acc, gate_acc), (all_gate, all_up, all_down) = lax.scan(one_expert, start_carry, (by_expert, gate_full, up_full, down_full))
    gate_grad = gate_acc.reshape(TOKENS, TOP)
    logit_grad = logit_grads(picked, weights, gate_grad)
    router_grad = jnp.dot(tokens.astype(jnp.float32).T, logit_grad, precision=highest)
    token_grad = (dx_acc.reshape(TOKENS, D) + jnp.dot(logit_grad, router.astype(jnp.float32).T, precision=highest)).astype(jnp.bfloat16)
    grad_gate = jnp.transpose(all_gate.reshape(EXPERTS, D, BLOCKS, half_ff), (0, 2, 1, 3)).reshape(EXPERTS * BLOCKS, D, half_ff)
    grad_up = jnp.transpose(all_up.reshape(EXPERTS, D, BLOCKS, half_ff), (0, 2, 1, 3)).reshape(EXPERTS * BLOCKS, D, half_ff)
    grad_down = all_down.reshape(EXPERTS * BLOCKS, half_ff, D)
    return (token_grad, gate_grad, grad_gate, grad_up, grad_down, router_grad)
```

```python
import jax
import jax.numpy as jnp
from jax import lax
from jax.experimental import pallas as pl
from jax.experimental.pallas import tpu as pltpu
from jax.sharding import PartitionSpec as P

BLOCKS = 2
CORES = 2
PLANES = 2
LINE = 4
PIECES = 2
MESH = pl.DeviceIdType.MESH


def build_slots(block_routes, experts, capacity):
    flat_routes = block_routes.reshape(-1)
    labels = jnp.arange(experts, dtype=jnp.int32)
    hit_mask = (flat_routes[None, :] == labels[:, None]).astype(jnp.int32)
    rank_in = jnp.cumsum(hit_mask, axis=1, dtype=jnp.int32) - 1
    slot_ids = jnp.arange(capacity, dtype=jnp.int32)
    assigned = (hit_mask[:, None, :] == 1) & (rank_in[:, None, :] == slot_ids[None, :, None])
    return assigned.astype(jnp.float32)


def gate_pair(tokens, routes, router, experts):
    logits = jnp.dot(tokens, router, preferred_element_type=jnp.float32)
    labels = jnp.arange(experts, dtype=jnp.int32)
    picked = (routes[:, :, None] == labels[None, None, :]).astype(jnp.float32)
    chosen = jnp.sum(picked * logits[:, None, :], axis=2)
    margin = chosen[:, 0] - chosen[:, 1]
    weights = jnp.stack([jax.nn.sigmoid(margin), jax.nn.sigmoid(-margin)], axis=1)
    return (picked, weights)


def logit_grads(picked, weights, gate_grad):
    lead_grad = weights[:, 0] * weights[:, 1] * (gate_grad[:, 0] - gate_grad[:, 1])
    pair_grad = jnp.stack([lead_grad, -lead_grad], axis=1)
    return jnp.sum(picked * pair_grad[:, :, None], axis=1)


def expert_grads(rows_in, cot_in, gate_in, gate_weight, up_weight, down_weight):
    pre_gate = jnp.dot(rows_in, gate_weight, preferred_element_type=jnp.float32)
    pre_up = jnp.dot(rows_in, up_weight, preferred_element_type=jnp.float32)
    back_grad = lax.dot_general(
        cot_in, down_weight, (((1,), (1,)), ((), ())), preferred_element_type=jnp.float32
    )
    sig_gate = jax.nn.sigmoid(pre_gate)
    active = pre_gate * sig_gate
    hidden = (active * pre_up).astype(jnp.bfloat16)
    gate_terms = jnp.sum(hidden.astype(jnp.float32) * back_grad, axis=1)
    gate_col = gate_in.astype(jnp.float32)[:, None]
    scaled_back = gate_col * back_grad
    d_gate = (scaled_back * pre_up * sig_gate * (1.0 + pre_gate * (1.0 - sig_gate))).astype(
        jnp.bfloat16
    )
    d_up = (scaled_back * active).astype(jnp.bfloat16)
    scaled_cot = (gate_col * cot_in.astype(jnp.float32)).astype(jnp.bfloat16)
    contract_rows = (((0,), (0,)), ((), ()))
    grad_gate = lax.dot_general(
        rows_in, d_gate, contract_rows, preferred_element_type=jnp.float32
    ).astype(jnp.bfloat16)
    grad_up = lax.dot_general(
        rows_in, d_up, contract_rows, preferred_element_type=jnp.float32
    ).astype(jnp.bfloat16)
    grad_down = lax.dot_general(
        hidden, scaled_cot, contract_rows, preferred_element_type=jnp.float32
    ).astype(jnp.bfloat16)
    return (d_gate, d_up, gate_terms, grad_gate, grad_up, grad_down)


def spread_slabs(packed, experts, slab_count):
    widened = jnp.broadcast_to(packed[:, None], (experts, BLOCKS) + packed.shape[1:])
    return widened.reshape((slab_count,) + packed.shape[1:])


def routed_shards(tokens, cotangent, routes, router, w_gate, w_up, w_down):
    highest = lax.Precision.HIGHEST
    ep_count = lax.axis_size("ep")
    tp_count = lax.axis_size("tp")
    experts = ep_count // BLOCKS
    tok_rows, width = tokens.shape
    top_count = routes.shape[1]
    capacity = 3 * tok_rows * top_count // (2 * experts)
    col_width = width // tp_count
    tp_index = lax.axis_index("tp")
    picked, weights = gate_pair(tokens, routes, router, experts)
    assigned = build_slots(routes, experts, capacity)
    per_token = jnp.sum(assigned.reshape(experts, capacity, tok_rows, top_count), axis=3)
    token_map = per_token.astype(jnp.bfloat16)
    gate_send = weights.astype(jnp.bfloat16)
    gate_slots = jnp.einsum(
        "ecj,j->ec", assigned, gate_send.astype(jnp.float32).reshape(-1), precision=highest
    ).astype(jnp.bfloat16)
    gate_out = spread_slabs(gate_slots, experts, ep_count)

    def pack_rows(source):
        packed = jnp.einsum(
            "ect,td->ecd", token_map, source, preferred_element_type=jnp.float32
        ).astype(jnp.bfloat16)
        return spread_slabs(packed, experts, ep_count)

    tok_part = lax.dynamic_slice_in_dim(tokens, tp_index * col_width, col_width, 1)
    cot_part = lax.dynamic_slice_in_dim(cotangent, tp_index * col_width, col_width, 1)
    recv_part, recv_cot_part, recv_gate = (
        lax.all_to_all(pack_rows(tok_part), "ep", split_axis=0, concat_axis=0, tiled=True),
        lax.all_to_all(pack_rows(cot_part), "ep", split_axis=0, concat_axis=0, tiled=True),
        lax.all_to_all(gate_out, "ep", split_axis=0, concat_axis=0, tiled=True),
    )
    recv_rows, recv_cot = (
        lax.all_gather(recv_part, "tp", axis=2, tiled=True),
        lax.all_gather(recv_cot_part, "tp", axis=2, tiled=True),
    )
    rows_in = recv_rows.reshape(-1, width)
    cot_in = recv_cot.reshape(-1, width)
    gate_in = recv_gate.reshape(-1)
    d_gate, d_up, gate_terms, grad_gate, grad_up, grad_down = expert_grads(
        rows_in, cot_in, gate_in, w_gate[0], w_up[0], w_down[0]
    )
    contract_hidden = (((1,), (1,)), ((), ()))
    partial_dx = lax.dot_general(
        d_gate, w_gate[0], contract_hidden, preferred_element_type=jnp.float32
    )
    partial_dx = partial_dx + lax.dot_general(
        d_up, w_up[0], contract_hidden, preferred_element_type=jnp.float32
    )
    summed_dx = lax.psum_scatter(
        partial_dx.reshape(ep_count, capacity, width).astype(jnp.bfloat16),
        "tp",
        scatter_dimension=2,
        tiled=True,
    ).astype(jnp.float32)
    gate_sums = lax.psum(gate_terms.reshape(ep_count, capacity), "tp")
    back_dx, back_gate = (
        lax.all_to_all(
            summed_dx.astype(jnp.bfloat16), "ep", split_axis=0, concat_axis=0, tiled=True
        ).astype(summed_dx.dtype),
        lax.all_to_all(
            gate_sums.astype(jnp.bfloat16), "ep", split_axis=0, concat_axis=0, tiled=True
        ).astype(gate_sums.dtype),
    )
    slab_dx = jnp.sum(back_dx.reshape(experts, BLOCKS, capacity, col_width), axis=1)
    routed_dx = jnp.einsum("ect,ecd->td", per_token, slab_dx, precision=highest)
    slab_gate = jnp.sum(back_gate.reshape(experts, BLOCKS, capacity), axis=1)
    gate_grad = jnp.einsum("ecj,ec->j", assigned, slab_gate, precision=highest).reshape(
        tok_rows, top_count
    )
    logit_grad = logit_grads(picked, weights, gate_grad)
    router_cols = lax.dynamic_slice_in_dim(router, tp_index * col_width, col_width, 0).astype(
        jnp.float32
    )
    token_grad = (routed_dx + jnp.dot(logit_grad, router_cols.T, precision=highest)).astype(
        jnp.bfloat16
    )
    seg_rows = tok_rows // tp_count
    own_rows = lax.dynamic_slice_in_dim(tokens, tp_index * seg_rows, seg_rows, 0).astype(
        jnp.float32
    )
    own_logit = lax.dynamic_slice_in_dim(logit_grad, tp_index * seg_rows, seg_rows, 0)
    router_grad = lax.psum_scatter(
        jnp.dot(own_rows.T, own_logit, precision=highest),
        ("ep", "tp"),
        scatter_dimension=0,
        tiled=True,
    )
    return (token_grad, gate_grad, grad_gate[None], grad_up[None], grad_down[None], router_grad)


class Place:
    def __init__(self):
        ep, self.tp = lax.axis_index("ep"), lax.axis_index("tp")
        self.z, self.x = ep // BLOCKS, ep % BLOCKS
        self.y, self.c = self.tp // CORES, self.tp % CORES
        self.pair = self.z + 1 - 2 * (self.z % 2)
        self.near = 2 - self.z // 2
        self.far = 3 * (1 - self.z // 2)
        self.rank = 3 - (self.z + 1) // 2 % 2
        self.lines = (self.pair, self.near, self.far)
        self.slots = (1, self.rank, self.rank)

    def device(self, z, x):
        return {"ep": z * BLOCKS + x, "tp": self.tp}

    def along(self, z):
        return self.device(z, self.x)

    def across(self):
        return self.device(self.z, 1 - self.x)

    def other_plane(self):
        return {"ep": self.z * BLOCKS + self.x, "tp": (1 - self.y) * CORES + self.c}

    def other_core(self):
        return {"ep": self.z * BLOCKS + self.x, "tp": self.y * CORES + 1 - self.c}

    def turned(self, step, flip):
        return self.device((self.z + step) % LINE, (self.x + flip) % BLOCKS)

    def greet(self):
        barrier = pltpu.get_barrier_semaphore()
        peers = [self.turned(step, flip) for step in range(LINE) for flip in range(2)][1:]
        peers += [self.other_plane(), self.other_core()]
        for peer in peers:
            pl.semaphore_signal(barrier, inc=1, device_id=peer, device_id_type=MESH)
        pl.semaphore_wait(barrier, len(peers))


SCHEDULE = (
    "X0", "Z1", "Y01", "Y10", "F0", "X1", "Z2", "Y11", "D0", "Y20", "A0", "F1", "X2", "Z3",
    "B0", "D1", "Y21", "Y30", "E0", "A1", "X3", "F2", "B1", "D2", "Y31", "E1", "A2", "F3", "G0",
    "D3", "G1", "B2", "A3", "G2", "E2", "W0", "B3", "G3", "W1", "E3", "W2", "G4", "T", "R",
)


def fused_kernel(
    tok_hbm, cot_hbm, routes_ref, router_ref, wg_hbm, wu_hbm, wd_hbm,
    tg_ref, gg_ref, gw_ref, gu_ref, gd_ref, rg_ref,
    src, wgu, wd, rows, pack, hot, gate_send, gate_recv, gate_col,
    hs, dgu, dx_send, dx_own, c_recv, y_send, y_recv, y_own, x_send, x_recv, z_send, z_recv,
    g_sum, g_send, g_recv, gz_recv, r_send, r_recv,
    load_sems, z_sems, x_sems, y_sems, c_sems, gz_sems, gx_sems,
    sc_sems, sy_sems, sx_sems, sz_sems, gp_sems, gl_sems, r_sems,
):
    f32, bf16 = jnp.float32, jnp.bfloat16
    at = Place()
    cap, tok_rows, width = pack.shape[1], src.shape[1], src.shape[2]
    hidden, part = wd.shape[0], tg_ref.shape[1]
    span = pack.shape[2]
    rest = width - span
    size = cap // PIECES
    window = pl.ds(pl.multiple_of(at.y * rest, 128), span)
    outer = pl.ds(pl.multiple_of(at.y * span, 128), rest)
    inner = pl.ds(pl.multiple_of((1 - at.y) * span, 128), rest)
    started = []

    def dot(lhs, rhs, dims):
        return lax.dot_general(lhs, rhs, (dims, ((), ())), preferred_element_type=f32)

    def send(source, target, send_sem, recv_sem, peer):
        copy = pltpu.make_async_remote_copy(
            src_ref=source, dst_ref=target, send_sem=send_sem, recv_sem=recv_sem,
            device_id=peer, device_id_type=MESH,
        )
        copy.start()
        started.append(copy)

    def arrived(target, sem):
        pltpu.make_async_remote_copy(
            src_ref=target, dst_ref=target, send_sem=sem, recv_sem=sem,
            device_id=at.across(), device_id_type=MESH,
        ).wait_recv()

    loads = [
        pltpu.make_async_copy(tok_hbm, src.at[0], load_sems.at[0]),
        pltpu.make_async_copy(cot_hbm, src.at[1], load_sems.at[1]),
        pltpu.make_async_copy(wg_hbm, wgu.at[:, pl.ds(0, hidden)], load_sems.at[2]),
        pltpu.make_async_copy(wu_hbm, wgu.at[:, pl.ds(hidden, hidden)], load_sems.at[3]),
        pltpu.make_async_copy(wd_hbm, wd, load_sems.at[4]),
    ]
    for copy in loads:
        copy.start()

    side = hot.shape[1]
    row8 = lax.broadcasted_iota(jnp.int32, (8, tok_rows), 0)
    first, second = routes_ref[0:1, :], routes_ref[1:2, :]
    is_first, is_second = first == row8, second == row8
    hit = jnp.where(is_first | is_second, 1.0, 0.0)
    up_to = lax.broadcasted_iota(jnp.int32, (tok_rows, tok_rows), 0) <= lax.broadcasted_iota(
        jnp.int32, (tok_rows, tok_rows), 1
    )
    place = dot(hit, jnp.where(up_to, 1.0, 0.0), ((1,), (0,)))
    place = jnp.where(hit > 0.0, place, 0.0)
    slot = (lax.broadcasted_iota(jnp.int32, (side, tok_rows), 0) + 1).astype(f32)
    for e in range(LINE):
        hot[e] = jnp.where(slot == place[e : e + 1, :], 1.0, 0.0).astype(bf16)
    at.greet()

    loads[0].wait()
    loads[1].wait()

    def piece(k, j, h):
        return pl.ds((k * BLOCKS + j) * cap + h * size, size)

    def chunk(k):
        return slice(k * BLOCKS * cap, (k + 1) * BLOCKS * cap)

    def pass_x(k, h):
        send(
            rows.at[at.c, piece(k, 0, h), window], rows.at[at.c, piece(k, 1, h), window],
            x_sems.at[0, k, h], x_sems.at[1, k, h], at.across(),
        )

    def pass_y(k, j, h):
        ref = rows.at[at.c, piece(k, j, h), outer]
        send(ref, ref, y_sems.at[0, k, j, h], y_sems.at[1, k, j, h], at.other_plane())

    def pass_c(k, j, h):
        ref = rows.at[at.c, piece(k, j, h), :]
        send(ref, ref, c_sems.at[0, k, j, h], c_sems.at[1, k, j, h], at.other_core())

    own_hot = hot[at.z, 0:cap, :]
    rows[at.c, 0:cap, :] = dot(own_hot, src[at.c], ((1,), (0,))).astype(bf16)
    for h in range(PIECES):
        pass_x(0, h)
    for m in range(LINE - 1):
        pack[m] = dot(
            hot[at.lines[m], 0:cap, :], src[at.c, :, window], ((1,), (0,))
        ).astype(bf16)
        for h in range(PIECES):
            send(
                pack.at[m, pl.ds(h * size, size), :],
                rows.at[at.c, pl.ds(pl.multiple_of(at.slots[m] * BLOCKS * cap + h * size, 16), size), window],
                z_sems.at[0, m, h], z_sems.at[1, at.slots[m], h], at.along(at.lines[m]),
            )

    router = router_ref[...]
    logits = dot(router.astype(bf16), src[0], ((1,), (1,)))
    chosen = [
        jnp.sum(jnp.where(mask, logits, 0.0), axis=0, keepdims=True)
        for mask in (is_first, is_second)
    ]
    margin = chosen[0] - chosen[1]
    weights = [jax.nn.sigmoid(margin), jax.nn.sigmoid(-margin)]
    sent = [w.astype(bf16).astype(f32) for w in weights]
    by_expert = jnp.where(is_first, sent[0], 0.0) + jnp.where(is_second, sent[1], 0.0)
    for m, z in enumerate((at.z,) + at.lines):
        gate_send[m] = dot(by_expert.astype(bf16), hot[z], ((1,), (1,)))
    gate_recv[0] = gate_send[0]
    send(gate_send.at[0], gate_recv.at[1], gx_sems.at[0, 0], gx_sems.at[1, 0], at.across())
    for m in range(LINE - 1):
        send(
            gate_send.at[m + 1], gate_recv.at[at.slots[m] * BLOCKS],
            gz_sems.at[0, m], gz_sems.at[1, at.slots[m]], at.along(at.lines[m]),
        )
    rows[1 - at.c, 0:cap, :] = dot(own_hot, src[1 - at.c], ((1,), (0,))).astype(bf16)
    g_sum[...] = jnp.zeros_like(g_sum)

    row_id = lax.broadcasted_iota(jnp.int32, (side, side), 0)
    lane_id = lax.broadcasted_iota(jnp.int32, (side, side), 1)
    top8 = lax.broadcasted_iota(jnp.int32, (8, side), 0)
    diagonal = row_id == lane_id

    def to_column(row):
        return jnp.sum(jnp.where(diagonal, row, 0.0), axis=1, keepdims=True)

    def take_row(tile, index):
        return jnp.sum(jnp.where(top8 == index, tile, 0.0), axis=0, keepdims=True)

    sources = (at.z,) + at.lines

    def step_z(k):
        for h in range(PIECES):
            arrived(rows.at[at.c, piece(k, 0, h), window], z_sems.at[1, k, h])
            pass_x(k, h)
            pass_y(k, 0, h)
        arrived(gate_recv.at[k * BLOCKS], gz_sems.at[1, k])
        send(
            gate_recv.at[k * BLOCKS], gate_recv.at[k * BLOCKS + 1],
            gx_sems.at[0, k], gx_sems.at[1, k], at.across(),
        )

    def step_x(k):
        for h in range(PIECES):
            arrived(rows.at[at.c, piece(k, 1, h), window], x_sems.at[1, k, h])
            pass_y(k, 1, h)

    def step_y(k, j):
        for h in range(PIECES):
            arrived(rows.at[at.c, piece(k, j, h), inner], y_sems.at[1, k, j, h])
            pass_c(k, j, h)

    def forward(k):
        arrived(gate_recv.at[k * BLOCKS + 1], gx_sems.at[1, k])
        for j in range(BLOCKS):
            column = to_column(take_row(gate_recv[k * BLOCKS + j], at.z))
            base = (k * BLOCKS + j) * cap
            gate_col[base : base + cap, :] = jnp.broadcast_to(column[0:cap], (cap, side))
        for j in range(BLOCKS):
            if (k, j) != (0, 0):
                for h in range(PIECES):
                    arrived(rows.at[1 - at.c, piece(k, j, h), :], c_sems.at[1, k, j, h])
        if k == 0:
            for copy in loads[2:]:
                copy.wait()
        both = dot(rows[0, chunk(k), :], wgu[...], ((1,), (0,)))
        pre_gate, pre_up = both[:, :hidden], both[:, hidden:]
        back = dot(rows[1, chunk(k), :], wd[...], ((1,), (1,)))
        gate = gate_col[chunk(k), 0:1]
        sig = jax.nn.sigmoid(pre_gate)
        active = pre_gate * sig
        product = active * pre_up
        terms = jnp.sum(product.astype(bf16).astype(f32) * back, axis=1, keepdims=True)
        scaled = gate * back
        dgu[chunk(k), 0:hidden] = (scaled * pre_up * sig * (1.0 + pre_gate * (1.0 - sig))).astype(bf16)
        dgu[chunk(k), hidden:] = (scaled * active).astype(bf16)
        hs[chunk(k), :] = (gate * product).astype(bf16)
        for j in range(BLOCKS):
            line = jnp.sum(
                jnp.where(diagonal[0:cap], terms[j * cap : (j + 1) * cap], 0.0),
                axis=0, keepdims=True,
            )
            block = sources[k] * BLOCKS + (at.x if j == 0 else 1 - at.x)
            g_sum[...] += jnp.where(top8 == block, line, 0.0)

    def input_grad(k, plane, core):
        begin = pl.multiple_of((plane * CORES + core) * part, part)
        return dot(dgu[chunk(k), :], wgu[pl.ds(begin, part), :], ((1,), (1,)))

    def backward(k):
        for p in range(PLANES):
            dx_send[k, p] = input_grad(k, p, 1 - at.c).astype(bf16)
            send(
                dx_send.at[k, p], c_recv.at[k, p],
                sc_sems.at[0, k, p], sc_sems.at[1, k, p], at.other_core(),
            )
        for n, plane in enumerate((1 - at.y, at.y)):
            dx_own[k, n] = input_grad(k, plane, at.c)

    def after_c(k):
        for p in range(PLANES):
            arrived(c_recv.at[k, p], sc_sems.at[1, k, p])
        for j in (1, 0):
            part_rows = slice(j * cap, (j + 1) * cap)
            y_send[k, j] = (
                dx_own[k, 0, part_rows, :] + c_recv[k, 1 - at.y, part_rows, :].astype(f32)
            ).astype(bf16)
            send(
                y_send.at[k, j], y_recv.at[k, j],
                sy_sems.at[0, k, j], sy_sems.at[1, k, j], at.other_plane(),
            )
        for j in (1, 0):
            part_rows = slice(j * cap, (j + 1) * cap)
            y_own[k, j] = dx_own[k, 1, part_rows, :] + c_recv[k, at.y, part_rows, :].astype(f32)

    def after_y(k):
        arrived(y_recv.at[k, 1], sy_sems.at[1, k, 1])
        x_send[k] = (y_own[k, 1] + y_recv[k, 1].astype(f32)).astype(bf16)
        send(x_send.at[k], x_recv.at[k], sx_sems.at[0, k], sx_sems.at[1, k], at.across())
        arrived(y_recv.at[k, 0], sy_sems.at[1, k, 0])
        y_own[k, 0] = y_own[k, 0] + y_recv[k, 0].astype(f32)

    def after_x(k):
        arrived(x_recv.at[k], sx_sems.at[1, k])
        total = (y_own[k, 0] + x_recv[k].astype(f32)).astype(bf16)
        if k == 0:
            z_recv[at.z] = total
            return
        z_send[k - 1] = total
        mine = 1 if k == 1 else at.rank
        send(
            z_send.at[k - 1], z_recv.at[at.z],
            sz_sems.at[0, k], sz_sems.at[1, mine], at.along(sources[k]),
        )

    stages = (at.other_core, at.other_plane, at.across)

    def gate_stage(n):
        if n > 0:
            arrived(g_recv.at[n - 1], gp_sems.at[1, n - 1])
            g_sum[...] += g_recv[n - 1]
        if n < len(stages):
            g_send[n] = g_sum[...]
            send(g_send.at[n], g_recv.at[n], gp_sems.at[0, n], gp_sems.at[1, n], stages[n]())
            return
        g_send[n] = g_sum[...]
        gz_recv[at.z] = g_sum[...]
        for m in range(LINE - 1):
            send(
                g_send.at[n], gz_recv.at[at.z],
                gl_sems.at[0, m], gl_sems.at[1, at.slots[m]], at.along(at.lines[m]),
            )

    state = {}

    def split3(value):
        high = value.astype(bf16).astype(f32)
        middle = (value - high).astype(bf16).astype(f32)
        low = (value - high - middle).astype(bf16).astype(f32)
        return jnp.concatenate([high, middle, low, jnp.zeros_like(value)], axis=0).astype(bf16)

    def gate_finish():
        for m in range(LINE - 1):
            arrived(gz_recv.at[at.lines[m]], gl_sems.at[1, m + 1])
        own = at.z * BLOCKS + at.x
        grads = [jnp.zeros((1, tok_rows), f32)] * 2
        for e in range(LINE):
            column = to_column(take_row(gz_recv[e], own))
            term = jnp.sum(column * hot[e].astype(f32), axis=0, keepdims=True)
            grads[0] = grads[0] + jnp.where(first == e, term, 0.0)
            grads[1] = grads[1] + jnp.where(second == e, term, 0.0)
        gg_ref[...] = jnp.where(row8 == 0, grads[0], jnp.where(row8 == 1, grads[1], 0.0))
        lead = weights[0] * weights[1] * (grads[0] - grads[1])
        logit_grad = jnp.where(is_first, lead, 0.0) - jnp.where(is_second, lead, 0.0)
        state["parts"] = split3(logit_grad)
        sums = dot(state["parts"], src[0], ((1,), (0,)))
        r_send[...] = sums[0:8] + sums[8:16] + sums[16:24]
        wide = r_send.shape[1] // (LINE * BLOCKS)
        for step in range(LINE):
            for flip in range(BLOCKS):
                z, x = (at.z + step) % LINE, (at.x + flip) % BLOCKS
                columns = pl.ds(pl.multiple_of((z * BLOCKS + x) * wide, wide), wide)
                n = step * BLOCKS + flip
                if n == 0:
                    r_recv[0] = r_send[:, columns]
                    continue
                send(
                    r_send.at[:, columns], r_recv.at[n],
                    r_sems.at[0, n], r_sems.at[1, n], at.device(z, x),
                )

    def token_finish():
        begin = pl.multiple_of(at.tp * part, part)
        columns = router_ref[:, pl.ds(begin, part)]
        triple = jnp.concatenate([columns] * 3 + [jnp.zeros_like(columns)], axis=0).astype(bf16)
        total = dot(state["parts"], triple, ((0,), (0,)))
        for m in range(LINE - 1):
            arrived(z_recv.at[at.lines[m]], sz_sems.at[1, m + 1])
        for e in range(LINE):
            total = total + dot(hot[e, 0:cap, :], z_recv[e], ((0,), (0,)))
        tg_ref[...] = total.astype(bf16)

    def router_finish():
        total = r_recv[0]
        for n in range(1, LINE * BLOCKS):
            arrived(r_recv.at[n], r_sems.at[1, n])
            total = total + r_recv[n]
        rg_ref[...] = total

    tile = 256

    def weight_grads(n):
        if n < 2:
            half = width // tile // 2

            @pl.loop(n * half, (n + 1) * half)
            def _(m):
                columns = pl.ds(pl.multiple_of(m * tile, tile), tile)
                both = dot(rows[0, :, columns], dgu[...], ((0,), (0,))).astype(bf16)
                gw_ref[columns, :] = both[:, :hidden]
                gu_ref[columns, :] = both[:, hidden:]

            return

        @pl.loop(0, width // tile)
        def _(m):
            columns = pl.ds(pl.multiple_of(m * tile, tile), tile)
            gd_ref[:, columns] = dot(hs[...], rows[1, :, columns], ((0,), (0,))).astype(bf16)

    steps = {
        "X": step_x, "Z": step_z, "Y": step_y, "F": forward, "D": backward, "A": after_c,
        "B": after_y, "E": after_x, "W": weight_grads, "T": token_finish, "R": router_finish,
    }
    for token in SCHEDULE:
        numbers = [int(digit) for digit in token[1:]]
        if token[0] == "G":
            gate_stage(*numbers) if numbers[0] <= len(stages) else gate_finish()
        else:
            steps[token[0]](*numbers)
    for copy in started:
        copy.wait_send()


def fused_shards(tokens, cotangent, routes, router, w_gate, w_up, w_down):
    ep_count, tp_count = lax.axis_size("ep"), lax.axis_size("tp")
    experts = ep_count // BLOCKS
    tok_rows, width = tokens.shape
    cap = 3 * tok_rows * routes.shape[1] // (2 * experts)
    part, hidden = width // tp_count, w_down.shape[1]
    span = 5 * width // 8
    seg = width // (ep_count * tp_count)
    routes_t = jnp.pad(routes.T, ((0, 8 - routes.shape[1]), (0, 0)))
    router_t = jnp.pad(router.T.astype(jnp.float32), ((0, 8 - experts), (0, 0)))
    dma = pltpu.SemaphoreType.DMA
    bf16, f32 = jnp.bfloat16, jnp.float32
    vmem = pl.BlockSpec(memory_space=pltpu.VMEM)
    anywhere = pl.BlockSpec(memory_space=pl.ANY)
    total, pair = ep_count * cap, BLOCKS * cap
    tiny = (8, 128)
    token_grad, gates, grad_gate, grad_up, grad_down, router_grad = pl.pallas_call(
        fused_kernel,
        out_shape=(
            jax.ShapeDtypeStruct((tok_rows, part), bf16),
            jax.ShapeDtypeStruct((8, tok_rows), f32),
            jax.ShapeDtypeStruct((width, hidden), bf16),
            jax.ShapeDtypeStruct((width, hidden), bf16),
            jax.ShapeDtypeStruct((hidden, width), bf16),
            jax.ShapeDtypeStruct((8, width // ep_count), f32),
        ),
        in_specs=[anywhere, anywhere, vmem, vmem, anywhere, anywhere, anywhere],
        out_specs=[vmem] * 6,
        scratch_shapes=[
            pltpu.VMEM((2, tok_rows, width), bf16),
            pltpu.VMEM((width, 2 * hidden), bf16),
            pltpu.VMEM((hidden, width), bf16),
            pltpu.VMEM((2, total, width), bf16),
            pltpu.VMEM((LINE - 1, cap, span), bf16),
            pltpu.VMEM((LINE, 128, tok_rows), bf16),
            pltpu.VMEM((LINE,) + tiny, f32),
            pltpu.VMEM((ep_count,) + tiny, f32),
            pltpu.VMEM((total, 128), f32),
            pltpu.VMEM((total, hidden), bf16),
            pltpu.VMEM((total, 2 * hidden), bf16),
            pltpu.VMEM((LINE, PLANES, pair, part), bf16),
            pltpu.VMEM((LINE, PLANES, pair, part), f32),
            pltpu.VMEM((LINE, PLANES, pair, part), bf16),
            pltpu.VMEM((LINE, BLOCKS, cap, part), bf16),
            pltpu.VMEM((LINE, BLOCKS, cap, part), bf16),
            pltpu.VMEM((LINE, BLOCKS, cap, part), f32),
            pltpu.VMEM((LINE, cap, part), bf16),
            pltpu.VMEM((LINE, cap, part), bf16),
            pltpu.VMEM((LINE - 1, cap, part), bf16),
            pltpu.VMEM((LINE, cap, part), bf16),
            pltpu.VMEM(tiny, f32),
            pltpu.VMEM((4,) + tiny, f32),
            pltpu.VMEM((3,) + tiny, f32),
            pltpu.VMEM((LINE,) + tiny, f32),
            pltpu.VMEM((8, width), f32),
            pltpu.VMEM((ep_count, 8, width // ep_count), f32),
            dma((5,)),
            dma((2, LINE, PIECES)),
            dma((2, LINE, PIECES)),
            dma((2, LINE, BLOCKS, PIECES)),
            dma((2, LINE, BLOCKS, PIECES)),
            dma((2, LINE)),
            dma((2, LINE)),
            dma((2, LINE, PLANES)),
            dma((2, LINE, BLOCKS)),
            dma((2, LINE)),
            dma((2, LINE)),
            dma((2, 3)),
            dma((2, LINE)),
            dma((2, ep_count)),
        ],
        compiler_params=pltpu.CompilerParams(
            collective_id=0, has_side_effects=True, vmem_limit_bytes=60 * 1024 * 1024
        ),
    )(tokens, cotangent, routes_t, router_t, w_gate[0], w_up[0], w_down[0])
    own = lax.dynamic_slice_in_dim(router_grad, lax.axis_index("tp") * seg, seg, 1)
    return (
        token_grad,
        gates[: routes.shape[1]].T,
        grad_gate[None],
        grad_up[None],
        grad_down[None],
        own[:experts].T,
    )


def shards(tokens, cotangent, routes, router, w_gate, w_up, w_down):
    grid = (lax.axis_size("ep"), lax.axis_size("tp"))
    path = fused_shards if grid == (LINE * BLOCKS, PLANES * CORES) else routed_shards
    return path(tokens, cotangent, routes, router, w_gate, w_up, w_down)


def solution(mesh):
    placed = (
        P("ep", None),
        P("ep", None),
        P("ep", None),
        P(),
        P("ep", None, "tp"),
        P("ep", None, "tp"),
        P("ep", "tp", None),
    )
    return jax.shard_map(
        shards,
        mesh=mesh,
        in_specs=placed,
        out_specs=(
            P("ep", "tp"),
            P("ep", None),
            P("ep", None, "tp"),
            P("ep", None, "tp"),
            P("ep", "tp", None),
            P(("ep", "tp"), None),
        ),
        check_vma=False,
    )
```

```python
import jax
import jax.numpy as jnp
from jax import lax
from jax.experimental import pallas as pl
from jax.experimental.pallas import tpu as pltpu
from jax.sharding import PartitionSpec as P

BLOCKS = 2
CORES = 2
PLANES = 2
LINE = 4
PIECES = 2
SIXTEENTHS = 10
VMEM_LIMIT = 40 * 1024 * 1024
MESH = pl.DeviceIdType.MESH


def build_slots(block_routes, experts, capacity):
    flat_routes = block_routes.reshape(-1)
    labels = jnp.arange(experts, dtype=jnp.int32)
    hit_mask = (flat_routes[None, :] == labels[:, None]).astype(jnp.int32)
    rank_in = jnp.cumsum(hit_mask, axis=1, dtype=jnp.int32) - 1
    slot_ids = jnp.arange(capacity, dtype=jnp.int32)
    assigned = (hit_mask[:, None, :] == 1) & (rank_in[:, None, :] == slot_ids[None, :, None])
    return assigned.astype(jnp.float32)


def gate_pair(tokens, routes, router, experts):
    logits = jnp.dot(tokens, router, preferred_element_type=jnp.float32)
    labels = jnp.arange(experts, dtype=jnp.int32)
    picked = (routes[:, :, None] == labels[None, None, :]).astype(jnp.float32)
    chosen = jnp.sum(picked * logits[:, None, :], axis=2)
    margin = chosen[:, 0] - chosen[:, 1]
    weights = jnp.stack([jax.nn.sigmoid(margin), jax.nn.sigmoid(-margin)], axis=1)
    return (picked, weights)


def logit_grads(picked, weights, gate_grad):
    lead_grad = weights[:, 0] * weights[:, 1] * (gate_grad[:, 0] - gate_grad[:, 1])
    pair_grad = jnp.stack([lead_grad, -lead_grad], axis=1)
    return jnp.sum(picked * pair_grad[:, :, None], axis=1)


def expert_grads(rows_in, cot_in, gate_in, gate_weight, up_weight, down_weight):
    pre_gate = jnp.dot(rows_in, gate_weight, preferred_element_type=jnp.float32)
    pre_up = jnp.dot(rows_in, up_weight, preferred_element_type=jnp.float32)
    back_grad = lax.dot_general(
        cot_in, down_weight, (((1,), (1,)), ((), ())), preferred_element_type=jnp.float32
    )
    sig_gate = jax.nn.sigmoid(pre_gate)
    active = pre_gate * sig_gate
    hidden = (active * pre_up).astype(jnp.bfloat16)
    gate_terms = jnp.sum(hidden.astype(jnp.float32) * back_grad, axis=1)
    gate_col = gate_in.astype(jnp.float32)[:, None]
    scaled_back = gate_col * back_grad
    d_gate = (scaled_back * pre_up * sig_gate * (1.0 + pre_gate * (1.0 - sig_gate))).astype(
        jnp.bfloat16
    )
    d_up = (scaled_back * active).astype(jnp.bfloat16)
    scaled_cot = (gate_col * cot_in.astype(jnp.float32)).astype(jnp.bfloat16)
    contract_rows = (((0,), (0,)), ((), ()))
    grad_gate = lax.dot_general(
        rows_in, d_gate, contract_rows, preferred_element_type=jnp.float32
    ).astype(jnp.bfloat16)
    grad_up = lax.dot_general(
        rows_in, d_up, contract_rows, preferred_element_type=jnp.float32
    ).astype(jnp.bfloat16)
    grad_down = lax.dot_general(
        hidden, scaled_cot, contract_rows, preferred_element_type=jnp.float32
    ).astype(jnp.bfloat16)
    return (d_gate, d_up, gate_terms, grad_gate, grad_up, grad_down)


def spread_slabs(packed, experts, slab_count):
    widened = jnp.broadcast_to(packed[:, None], (experts, BLOCKS) + packed.shape[1:])
    return widened.reshape((slab_count,) + packed.shape[1:])


def routed_shards(tokens, cotangent, routes, router, w_gate, w_up, w_down):
    highest = lax.Precision.HIGHEST
    ep_count = lax.axis_size("ep")
    tp_count = lax.axis_size("tp")
    experts = ep_count // BLOCKS
    tok_rows, width = tokens.shape
    top_count = routes.shape[1]
    capacity = 3 * tok_rows * top_count // (2 * experts)
    col_width = width // tp_count
    tp_index = lax.axis_index("tp")
    picked, weights = gate_pair(tokens, routes, router, experts)
    assigned = build_slots(routes, experts, capacity)
    per_token = jnp.sum(assigned.reshape(experts, capacity, tok_rows, top_count), axis=3)
    token_map = per_token.astype(jnp.bfloat16)
    gate_send = weights.astype(jnp.bfloat16)
    gate_slots = jnp.einsum(
        "ecj,j->ec", assigned, gate_send.astype(jnp.float32).reshape(-1), precision=highest
    ).astype(jnp.bfloat16)
    gate_out = spread_slabs(gate_slots, experts, ep_count)

    def pack_rows(source):
        packed = jnp.einsum(
            "ect,td->ecd", token_map, source, preferred_element_type=jnp.float32
        ).astype(jnp.bfloat16)
        return spread_slabs(packed, experts, ep_count)

    tok_part = lax.dynamic_slice_in_dim(tokens, tp_index * col_width, col_width, 1)
    cot_part = lax.dynamic_slice_in_dim(cotangent, tp_index * col_width, col_width, 1)
    recv_part, recv_cot_part, recv_gate = (
        lax.all_to_all(pack_rows(tok_part), "ep", split_axis=0, concat_axis=0, tiled=True),
        lax.all_to_all(pack_rows(cot_part), "ep", split_axis=0, concat_axis=0, tiled=True),
        lax.all_to_all(gate_out, "ep", split_axis=0, concat_axis=0, tiled=True),
    )
    recv_rows, recv_cot = (
        lax.all_gather(recv_part, "tp", axis=2, tiled=True),
        lax.all_gather(recv_cot_part, "tp", axis=2, tiled=True),
    )
    rows_in = recv_rows.reshape(-1, width)
    cot_in = recv_cot.reshape(-1, width)
    gate_in = recv_gate.reshape(-1)
    d_gate, d_up, gate_terms, grad_gate, grad_up, grad_down = expert_grads(
        rows_in, cot_in, gate_in, w_gate[0], w_up[0], w_down[0]
    )
    contract_hidden = (((1,), (1,)), ((), ()))
    partial_dx = lax.dot_general(
        d_gate, w_gate[0], contract_hidden, preferred_element_type=jnp.float32
    )
    partial_dx = partial_dx + lax.dot_general(
        d_up, w_up[0], contract_hidden, preferred_element_type=jnp.float32
    )
    summed_dx = lax.psum_scatter(
        partial_dx.reshape(ep_count, capacity, width).astype(jnp.bfloat16),
        "tp",
        scatter_dimension=2,
        tiled=True,
    ).astype(jnp.float32)
    gate_sums = lax.psum(gate_terms.reshape(ep_count, capacity), "tp")
    back_dx, back_gate = (
        lax.all_to_all(
            summed_dx.astype(jnp.bfloat16), "ep", split_axis=0, concat_axis=0, tiled=True
        ).astype(summed_dx.dtype),
        lax.all_to_all(
            gate_sums.astype(jnp.bfloat16), "ep", split_axis=0, concat_axis=0, tiled=True
        ).astype(gate_sums.dtype),
    )
    slab_dx = jnp.sum(back_dx.reshape(experts, BLOCKS, capacity, col_width), axis=1)
    routed_dx = jnp.einsum("ect,ecd->td", per_token, slab_dx, precision=highest)
    slab_gate = jnp.sum(back_gate.reshape(experts, BLOCKS, capacity), axis=1)
    gate_grad = jnp.einsum("ecj,ec->j", assigned, slab_gate, precision=highest).reshape(
        tok_rows, top_count
    )
    logit_grad = logit_grads(picked, weights, gate_grad)
    router_cols = lax.dynamic_slice_in_dim(router, tp_index * col_width, col_width, 0).astype(
        jnp.float32
    )
    token_grad = (routed_dx + jnp.dot(logit_grad, router_cols.T, precision=highest)).astype(
        jnp.bfloat16
    )
    seg_rows = tok_rows // tp_count
    own_rows = lax.dynamic_slice_in_dim(tokens, tp_index * seg_rows, seg_rows, 0).astype(
        jnp.float32
    )
    own_logit = lax.dynamic_slice_in_dim(logit_grad, tp_index * seg_rows, seg_rows, 0)
    router_grad = lax.psum_scatter(
        jnp.dot(own_rows.T, own_logit, precision=highest),
        ("ep", "tp"),
        scatter_dimension=0,
        tiled=True,
    )
    return (token_grad, gate_grad, grad_gate[None], grad_up[None], grad_down[None], router_grad)


class Place:
    def __init__(self):
        ep, self.tp = lax.axis_index("ep"), lax.axis_index("tp")
        self.z, self.x = ep // BLOCKS, ep % BLOCKS
        self.y, self.c = self.tp // CORES, self.tp % CORES
        self.pair = self.z + 1 - 2 * (self.z % 2)
        self.near = 2 - self.z // 2
        self.far = 3 * (1 - self.z // 2)
        self.rank = 3 - (self.z + 1) // 2 % 2
        self.lines = (self.pair, self.near, self.far)
        self.slots = (1, self.rank, self.rank)

    def device(self, z, x):
        return {"ep": z * BLOCKS + x, "tp": self.tp}

    def along(self, z):
        return self.device(z, self.x)

    def across(self):
        return self.device(self.z, 1 - self.x)

    def other_plane(self):
        return {"ep": self.z * BLOCKS + self.x, "tp": (1 - self.y) * CORES + self.c}

    def other_core(self):
        return {"ep": self.z * BLOCKS + self.x, "tp": self.y * CORES + 1 - self.c}

    def diagonal(self):
        return {"ep": self.z * BLOCKS + 1 - self.x, "tp": (1 - self.y) * CORES + self.c}

    def announce(self):
        peers = [self.along(z) for z in self.lines]
        peers += [self.across(), self.other_plane(), self.diagonal(), self.other_core()]
        for peer in peers:
            pl.semaphore_signal(
                pltpu.get_barrier_semaphore(), inc=1, device_id=peer, device_id_type=MESH
            )
        return len(peers)


SCHEDULE = (
    "X00", "Z10", "Z11", "X01", "X10", "Z20", "Y010", "Y011", "X11", "Z21", "X20", "Z30", "F0",
    "Y101", "X21", "D0", "Y110", "Z31", "Y201", "Y100", "A0", "Y111", "Y211", "Y200", "F1",
    "X30", "X31", "Y210", "Y300", "D1", "F2", "Y301", "A1", "D2", "Y310", "Y311", "A2", "F3",
    "G0", "D3", "E0", "E1", "G1", "A3", "W0", "G2", "E2", "W1", "E3", "G3", "R0", "W2", "T",
    "R1",
)


def fused_kernel(
    tok_hbm, cot_hbm, routes_hbm, router_hbm, wg_hbm, wu_hbm, wd_hbm,
    tg_ref, gg_ref, gw_ref, gu_ref, gd_ref, rg_ref,
    src, wgu, wd, rows, pack, hot, gate_send, gate_recv, gate_col,
    routes_ref, router_ref, router_all, hs, dgu, dx_send, dx_own, c_recv, s_send, s_recv, s_own, z_send, z_recv,
    g_sum, g_send, g_recv, gz_recv, r_send, r_recv, rz_send, rz_recv,
    load_sems, z_sems, x_sems, y_sems, c_sems, gz_sems, gx_sems,
    sc_sems, s_sems, sz_sems, gp_sems, gl_sems, r_sems,
):
    f32, bf16 = jnp.float32, jnp.bfloat16
    at = Place()
    cap, tok_rows, width = pack.shape[1], src.shape[1], src.shape[2]
    hidden, part = wd.shape[0], tg_ref.shape[1]
    span = pack.shape[2]
    rest = width - span
    size = cap // PIECES
    window = pl.ds(pl.multiple_of(at.y * rest, 128), span)
    outer = pl.ds(pl.multiple_of(at.y * span, 128), rest)
    inner = pl.ds(pl.multiple_of((1 - at.y) * span, 128), rest)
    started = []

    def dot(lhs, rhs, dims):
        return lax.dot_general(lhs, rhs, (dims, ((), ())), preferred_element_type=f32)

    def send(source, target, send_sem, recv_sem, peer):
        copy = pltpu.make_async_remote_copy(
            src_ref=source, dst_ref=target, send_sem=send_sem, recv_sem=recv_sem,
            device_id=peer, device_id_type=MESH,
        )
        copy.start()
        started.append(copy)

    def arrived(target, sem):
        pltpu.make_async_remote_copy(
            src_ref=target, dst_ref=target, send_sem=sem, recv_sem=sem,
            device_id=at.across(), device_id_type=MESH,
        ).wait_recv()

    greeted = at.announce()
    loads = [
        pltpu.make_async_copy(routes_hbm, routes_ref, load_sems.at[5]),
        pltpu.make_async_copy(tok_hbm, src.at[0], load_sems.at[0]),
        pltpu.make_async_copy(cot_hbm, src.at[1], load_sems.at[1]),
        pltpu.make_async_copy(router_hbm, router_ref, load_sems.at[6]),
        pltpu.make_async_copy(wg_hbm, wgu.at[:, pl.ds(0, hidden)], load_sems.at[2]),
        pltpu.make_async_copy(wu_hbm, wgu.at[:, pl.ds(hidden, hidden)], load_sems.at[3]),
        pltpu.make_async_copy(wd_hbm, wd, load_sems.at[4]),
    ]
    for copy in loads:
        copy.start()
    loads[0].wait()

    side = hot.shape[1]
    row8 = lax.broadcasted_iota(jnp.int32, (8, tok_rows), 0)
    first, second = routes_ref[0:1, :], routes_ref[1:2, :]
    is_first, is_second = first == row8, second == row8
    hit = jnp.where(is_first | is_second, 1.0, 0.0)
    up_to = lax.broadcasted_iota(jnp.int32, (tok_rows, tok_rows), 0) <= lax.broadcasted_iota(
        jnp.int32, (tok_rows, tok_rows), 1
    )
    place = dot(hit, jnp.where(up_to, 1.0, 0.0), ((1,), (0,)))
    place = jnp.where(hit > 0.0, place, 0.0)
    slot = (lax.broadcasted_iota(jnp.int32, (side, tok_rows), 0) + 1).astype(f32)
    for e in range(LINE):
        hot[e] = jnp.where(slot == place[e : e + 1, :], 1.0, 0.0).astype(bf16)
    loads[1].wait()
    loads[2].wait()

    def piece(k, j, h):
        return pl.ds((k * BLOCKS + j) * cap + h * size, size)

    def chunk(k):
        return slice(k * BLOCKS * cap, (k + 1) * BLOCKS * cap)

    def pass_x(k, h):
        send(
            rows.at[at.c, piece(k, 0, h), window], rows.at[at.c, piece(k, 1, h), window],
            x_sems.at[0, k, h], x_sems.at[1, k, h], at.across(),
        )

    def pass_y(k, j, h):
        ref = rows.at[at.c, piece(k, j, h), outer]
        send(ref, ref, y_sems.at[0, k, j, h], y_sems.at[1, k, j, h], at.other_plane())

    def pass_c(k, j, h):
        ref = rows.at[at.c, piece(k, j, h), :]
        send(ref, ref, c_sems.at[0, k, j, h], c_sems.at[1, k, j, h], at.other_core())

    own_hot = hot[at.z, 0:cap, :]
    rows[at.c, 0:cap, :] = dot(own_hot, src[at.c], ((1,), (0,))).astype(bf16)
    for m in range(LINE - 1):
        pack[m] = dot(
            hot[at.lines[m], 0:cap, :], src[at.c, :, window], ((1,), (0,))
        ).astype(bf16)
    pl.semaphore_wait(pltpu.get_barrier_semaphore(), greeted)
    for h in range(PIECES):
        pass_x(0, h)
    for m in range(LINE - 1):
        for h in range(PIECES):
            begin = pl.multiple_of(at.slots[m] * BLOCKS * cap + h * size, 16)
            send(
                pack.at[m, pl.ds(h * size, size), :],
                rows.at[at.c, pl.ds(begin, size), window],
                z_sems.at[0, m, h], z_sems.at[1, at.slots[m], h], at.along(at.lines[m]),
            )

    experts = router_ref.shape[0]
    loads[3].wait()
    router_all[0:experts, :] = router_ref[...].astype(f32)
    router_all[experts:, :] = jnp.zeros((8 - experts, width), f32)
    logits = dot(router_all[...].astype(bf16), src[0], ((1,), (1,)))
    chosen = [
        jnp.sum(jnp.where(mask, logits, 0.0), axis=0, keepdims=True)
        for mask in (is_first, is_second)
    ]
    margin = chosen[0] - chosen[1]
    weights = [jax.nn.sigmoid(margin), jax.nn.sigmoid(-margin)]
    sent = [w.astype(bf16).astype(f32) for w in weights]
    by_expert = jnp.where(is_first, sent[0], 0.0) + jnp.where(is_second, sent[1], 0.0)
    for m, z in enumerate((at.z,) + at.lines):
        gate_send[m] = dot(by_expert.astype(bf16), hot[z], ((1,), (1,)))
    gate_recv[0] = gate_send[0]
    send(gate_send.at[0], gate_recv.at[1], gx_sems.at[0, 0], gx_sems.at[1, 0], at.across())
    for m in range(LINE - 1):
        send(
            gate_send.at[m + 1], gate_recv.at[at.slots[m] * BLOCKS],
            gz_sems.at[0, m], gz_sems.at[1, at.slots[m]], at.along(at.lines[m]),
        )
    rows[1 - at.c, 0:cap, :] = dot(own_hot, src[1 - at.c], ((1,), (0,))).astype(bf16)
    g_sum[...] = jnp.zeros_like(g_sum)

    row_id = lax.broadcasted_iota(jnp.int32, (side, side), 0)
    lane_id = lax.broadcasted_iota(jnp.int32, (side, side), 1)
    top8 = lax.broadcasted_iota(jnp.int32, (8, side), 0)
    diagonal = row_id == lane_id

    def to_column(row):
        return jnp.sum(jnp.where(diagonal, row, 0.0), axis=1, keepdims=True)

    def take_row(tile, index):
        return jnp.sum(jnp.where(top8 == index, tile, 0.0), axis=0, keepdims=True)

    sources = (at.z,) + at.lines

    def step_z(k, h):
        arrived(rows.at[at.c, piece(k, 0, h), window], z_sems.at[1, k, h])
        pass_x(k, h)
        pass_y(k, 0, h)
        if h == 0:
            arrived(gate_recv.at[k * BLOCKS], gz_sems.at[1, k])
            send(
                gate_recv.at[k * BLOCKS], gate_recv.at[k * BLOCKS + 1],
                gx_sems.at[0, k], gx_sems.at[1, k], at.across(),
            )

    def step_x(k, h):
        arrived(rows.at[at.c, piece(k, 1, h), window], x_sems.at[1, k, h])
        pass_y(k, 1, h)

    def step_y(k, j, h):
        arrived(rows.at[at.c, piece(k, j, h), inner], y_sems.at[1, k, j, h])
        pass_c(k, j, h)

    def forward(k):
        arrived(gate_recv.at[k * BLOCKS + 1], gx_sems.at[1, k])
        for j in range(BLOCKS):
            column = to_column(take_row(gate_recv[k * BLOCKS + j], at.z))
            base = (k * BLOCKS + j) * cap
            gate_col[base : base + cap, :] = jnp.broadcast_to(column[0:cap], (cap, side))
        for j in range(BLOCKS):
            if (k, j) != (0, 0):
                for h in range(PIECES):
                    arrived(rows.at[1 - at.c, piece(k, j, h), :], c_sems.at[1, k, j, h])
        if k == 0:
            for copy in loads[4:]:
                copy.wait()
        both = dot(rows[0, chunk(k), :], wgu[...], ((1,), (0,)))
        pre_gate, pre_up = both[:, :hidden], both[:, hidden:]
        back = dot(rows[1, chunk(k), :], wd[...], ((1,), (1,)))
        gate = gate_col[chunk(k), 0:1]
        sig = jax.nn.sigmoid(pre_gate)
        active = pre_gate * sig
        product = active * pre_up
        terms = jnp.sum(product.astype(bf16).astype(f32) * back, axis=1, keepdims=True)
        scaled = gate * back
        dgu[chunk(k), 0:hidden] = (scaled * pre_up * sig * (1.0 + pre_gate * (1.0 - sig))).astype(bf16)
        dgu[chunk(k), hidden:] = (scaled * active).astype(bf16)
        hs[chunk(k), :] = (gate * product).astype(bf16)
        for j in range(BLOCKS):
            line = jnp.sum(
                jnp.where(diagonal[0:cap], terms[j * cap : (j + 1) * cap], 0.0),
                axis=0, keepdims=True,
            )
            block = sources[k] * BLOCKS + (at.x if j == 0 else 1 - at.x)
            g_sum[...] += jnp.where(top8 == block, line, 0.0)

    def input_grad(k, plane, core):
        begin = pl.multiple_of((plane * CORES + core) * part, part)
        return dot(dgu[chunk(k), :], wgu[pl.ds(begin, part), :], ((1,), (1,)))

    def backward(k):
        for p in range(PLANES):
            dx_send[k, p] = input_grad(k, p, 1 - at.c).astype(bf16)
            send(
                dx_send.at[k, p], c_recv.at[k, p],
                sc_sems.at[0, k, p], sc_sems.at[1, k, p], at.other_core(),
            )
        for n, plane in enumerate((1 - at.y, at.y)):
            dx_own[k, n] = input_grad(k, plane, at.c)

    def after_c(k):
        for p in range(PLANES):
            arrived(c_recv.at[k, p], sc_sems.at[1, k, p])

        def summed(n, plane, j):
            part_rows = slice(j * cap, (j + 1) * cap)
            return dx_own[k, n, part_rows, :] + c_recv[k, plane, part_rows, :].astype(f32)

        ways = (
            (0, 1 - at.y, 1, at.diagonal), (1, at.y, 1, at.across), (0, 1 - at.y, 0, at.other_plane),
        )
        for i, (n, plane, j, peer) in enumerate(ways):
            s_send[k, i] = summed(n, plane, j).astype(bf16)
            send(
                s_send.at[k, i], s_recv.at[k, i], s_sems.at[0, k, i], s_sems.at[1, k, i], peer()
            )
        s_own[k] = summed(1, at.y, 0)

    def after_x(k):
        total = s_own[k]
        for i in range(3):
            arrived(s_recv.at[k, i], s_sems.at[1, k, i])
            total = total + s_recv[k, i].astype(f32)
        total = total.astype(bf16)
        if k == 0:
            z_recv[at.z] = total
            return
        z_send[k - 1] = total
        mine = 1 if k == 1 else at.rank
        send(
            z_send.at[k - 1], z_recv.at[at.z],
            sz_sems.at[0, k], sz_sems.at[1, mine], at.along(sources[k]),
        )

    def gate_stage(n):
        if n == 0:
            send(g_sum, g_recv.at[0], gp_sems.at[0, 0], gp_sems.at[1, 0], at.other_core())
        elif n == 1:
            arrived(g_recv.at[0], gp_sems.at[1, 0])
            g_send[0] = g_sum[...] + g_recv[0]
            for i, peer in enumerate((at.across, at.other_plane, at.diagonal), 1):
                send(g_send.at[0], g_recv.at[i], gp_sems.at[0, i], gp_sems.at[1, i], peer())
        elif n == 2:
            total = g_send[0]
            for i in range(1, 4):
                arrived(g_recv.at[i], gp_sems.at[1, i])
                total = total + g_recv[i]
            g_send[1] = total
            gz_recv[at.z] = total
            for m in range(LINE - 1):
                send(
                    g_send.at[1], gz_recv.at[at.z],
                    gl_sems.at[0, m], gl_sems.at[1, at.slots[m]], at.along(at.lines[m]),
                )
        else:
            gate_finish()

    state = {}

    def split3(value):
        high = value.astype(bf16).astype(f32)
        middle = (value - high).astype(bf16).astype(f32)
        low = (value - high - middle).astype(bf16).astype(f32)
        return jnp.concatenate([high, middle, low, jnp.zeros_like(value)], axis=0).astype(bf16)

    def gate_finish():
        for m in range(LINE - 1):
            arrived(gz_recv.at[at.lines[m]], gl_sems.at[1, m + 1])
        own = at.z * BLOCKS + at.x
        grads = [jnp.zeros((1, tok_rows), f32)] * 2
        for e in range(LINE):
            column = to_column(take_row(gz_recv[e], own))
            term = jnp.sum(column * hot[e].astype(f32), axis=0, keepdims=True)
            grads[0] = grads[0] + jnp.where(first == e, term, 0.0)
            grads[1] = grads[1] + jnp.where(second == e, term, 0.0)
        gg_ref[...] = jnp.where(row8 == 0, grads[0], jnp.where(row8 == 1, grads[1], 0.0))
        lead = weights[0] * weights[1] * (grads[0] - grads[1])
        logit_grad = jnp.where(is_first, lead, 0.0) - jnp.where(is_second, lead, 0.0)
        state["parts"] = split3(logit_grad)
        sums = dot(state["parts"], src[0], ((1,), (0,)))
        sums = sums[0:8] + sums[8:16] + sums[16:24]
        wide = r_send.shape[3]
        for z in range(LINE):
            for x in range(BLOCKS):
                begin = (z * BLOCKS + x) * wide
                r_send[x, z] = sums[:, begin : begin + wide]
        send(r_send.at[1 - at.x], r_recv, r_sems.at[0, 0], r_sems.at[1, 0], at.across())

    def token_finish():
        begin = pl.multiple_of(at.tp * part, part)
        columns = router_all[:, pl.ds(begin, part)]
        triple = jnp.concatenate([columns] * 3 + [jnp.zeros_like(columns)], axis=0).astype(bf16)
        total = dot(state["parts"], triple, ((0,), (0,)))
        for m in range(LINE - 1):
            arrived(z_recv.at[at.lines[m]], sz_sems.at[1, m + 1])
        for e in range(LINE):
            total = total + dot(hot[e, 0:cap, :], z_recv[e], ((0,), (0,)))
        tg_ref[...] = total.astype(bf16)

    def router_stage(n):
        if n == 0:
            arrived(r_recv, r_sems.at[1, 0])
            rz_send[...] = r_send[at.x] + r_recv[...]
            for m in range(LINE - 1):
                send(
                    rz_send.at[at.lines[m]], rz_recv.at[at.slots[m] - 1],
                    r_sems.at[0, m + 1], r_sems.at[1, at.slots[m]], at.along(at.lines[m]),
                )
            return
        total = rz_send[at.z]
        for m in range(LINE - 1):
            arrived(rz_recv.at[m], r_sems.at[1, m + 1])
            total = total + rz_recv[m]
        seg = rg_ref.shape[1]
        own = jnp.zeros((8, seg), f32)
        for i in range(PLANES * CORES):
            own = jnp.where(at.tp == i, total[:, i * seg : (i + 1) * seg], own)
        rg_ref[...] = own

    tile = 256

    def weight_grads(n):
        if n < 2:
            half = width // tile // 2
            for m in range(n * half, (n + 1) * half):
                columns = slice(m * tile, (m + 1) * tile)
                both = dot(rows[0, :, columns], dgu[...], ((0,), (0,))).astype(bf16)
                gw_ref[columns, :] = both[:, :hidden]
                gu_ref[columns, :] = both[:, hidden:]
            return
        for m in range(hidden // tile):
            columns = slice(m * tile, (m + 1) * tile)
            gd_ref[columns, :] = dot(hs[:, columns], rows[1], ((0,), (0,))).astype(bf16)

    steps = {
        "X": step_x, "Z": step_z, "Y": step_y, "F": forward, "D": backward, "A": after_c,
        "E": after_x, "G": gate_stage, "W": weight_grads, "T": token_finish, "R": router_stage,
    }
    for token in SCHEDULE:
        steps[token[0]](*[int(digit) for digit in token[1:]])
    for copy in started:
        copy.wait_send()


def store_kernel(tg_in, gg_in, gw_in, gu_in, gd_in, rg_in, tg, gg, gw, gu, gd, rg, gates, router, sems):
    gates[...] = gg_in[0 : gates.shape[0], :]
    router[...] = rg_in[0 : router.shape[0], :]
    copies = []
    for source, target in ((gw_in, gw), (gu_in, gu), (gd_in, gd), (tg_in, tg), (gates, gg), (router, rg)):
        copies.append(pltpu.make_async_copy(source, target, sems.at[len(copies)]))
        copies[-1].start()
    for copy in copies:
        copy.wait()


def in_hbm(array):
    return pltpu.with_memory_space_constraint(array, pltpu.HBM)


def fused_shards(tokens, cotangent, routes, router, w_gate, w_up, w_down):
    ep_count, tp_count = lax.axis_size("ep"), lax.axis_size("tp")
    experts = ep_count // BLOCKS
    tok_rows, width = tokens.shape
    cap = 3 * tok_rows * routes.shape[1] // (2 * experts)
    part, hidden = width // tp_count, w_down.shape[1]
    span = SIXTEENTHS * width // 16
    seg, wide = width // (ep_count * tp_count), width // ep_count
    dma = pltpu.SemaphoreType.DMA
    bf16, f32 = jnp.bfloat16, jnp.float32
    vmem = pl.BlockSpec(memory_space=pltpu.VMEM)
    hbm = pl.BlockSpec(memory_space=pltpu.HBM)
    total, pair = ep_count * cap, BLOCKS * cap
    tiny = (8, 128)
    results = pl.pallas_call(
        fused_kernel,
        out_shape=(
            jax.ShapeDtypeStruct((tok_rows, part), bf16),
            jax.ShapeDtypeStruct((8, tok_rows), f32),
            jax.ShapeDtypeStruct((width, hidden), bf16),
            jax.ShapeDtypeStruct((width, hidden), bf16),
            jax.ShapeDtypeStruct((hidden, width), bf16),
            jax.ShapeDtypeStruct((8, seg), f32),
        ),
        in_specs=[hbm] * 7,
        out_specs=[vmem] * 6,
        scratch_shapes=[
            pltpu.VMEM((2, tok_rows, width), bf16),
            pltpu.VMEM((width, 2 * hidden), bf16),
            pltpu.VMEM((hidden, width), bf16),
            pltpu.VMEM((2, total, width), bf16),
            pltpu.VMEM((LINE - 1, cap, span), bf16),
            pltpu.VMEM((LINE, 128, tok_rows), bf16),
            pltpu.VMEM((LINE,) + tiny, f32),
            pltpu.VMEM((ep_count,) + tiny, f32),
            pltpu.VMEM((total, 128), f32),
            pltpu.VMEM((routes.shape[1], tok_rows), jnp.int32),
            pltpu.VMEM((experts, width), bf16),
            pltpu.VMEM((8, width), f32),
            pltpu.VMEM((total, hidden), bf16),
            pltpu.VMEM((total, 2 * hidden), bf16),
            pltpu.VMEM((LINE, PLANES, pair, part), bf16),
            pltpu.VMEM((LINE, PLANES, pair, part), f32),
            pltpu.VMEM((LINE, PLANES, pair, part), bf16),
            pltpu.VMEM((LINE, 3, cap, part), bf16),
            pltpu.VMEM((LINE, 3, cap, part), bf16),
            pltpu.VMEM((LINE, cap, part), f32),
            pltpu.VMEM((LINE - 1, cap, part), bf16),
            pltpu.VMEM((LINE, cap, part), bf16),
            pltpu.VMEM(tiny, f32),
            pltpu.VMEM((2,) + tiny, f32),
            pltpu.VMEM((4,) + tiny, f32),
            pltpu.VMEM((LINE,) + tiny, f32),
            pltpu.VMEM((BLOCKS, LINE, 8, wide), f32),
            pltpu.VMEM((LINE, 8, wide), f32),
            pltpu.VMEM((LINE, 8, wide), f32),
            pltpu.VMEM((LINE - 1, 8, wide), f32),
            dma((7,)),
            dma((2, LINE, PIECES)),
            dma((2, LINE, PIECES)),
            dma((2, LINE, BLOCKS, PIECES)),
            dma((2, LINE, BLOCKS, PIECES)),
            dma((2, LINE)),
            dma((2, LINE)),
            dma((2, LINE, PLANES)),
            dma((2, LINE, 3)),
            dma((2, LINE)),
            dma((2, 4)),
            dma((2, LINE)),
            dma((2, LINE)),
        ],
        compiler_params=pltpu.CompilerParams(
            collective_id=0, has_side_effects=True, vmem_limit_bytes=VMEM_LIMIT
        ),
    )(*map(in_hbm, (tokens, cotangent, routes.T, router.T, w_gate[0], w_up[0], w_down[0])))
    top = routes.shape[1]
    token_grad, gates, grad_gate, grad_up, grad_down, router_grad = pl.pallas_call(
        store_kernel,
        out_shape=(
            jax.ShapeDtypeStruct((tok_rows, part), bf16),
            jax.ShapeDtypeStruct((top, tok_rows), f32),
            jax.ShapeDtypeStruct((width, hidden), bf16),
            jax.ShapeDtypeStruct((width, hidden), bf16),
            jax.ShapeDtypeStruct((hidden, width), bf16),
            jax.ShapeDtypeStruct((experts, seg), f32),
        ),
        in_specs=[vmem] * 6,
        out_specs=[hbm] * 6,
        scratch_shapes=[
            pltpu.VMEM((top, tok_rows), f32),
            pltpu.VMEM((experts, seg), f32),
            dma((6,)),
        ],
        compiler_params=pltpu.CompilerParams(vmem_limit_bytes=16 * 1024 * 1024),
    )(*results)
    return (
        token_grad,
        gates.T,
        grad_gate[None],
        grad_up[None],
        grad_down[None],
        router_grad.T,
    )


def shards(tokens, cotangent, routes, router, w_gate, w_up, w_down):
    grid = (lax.axis_size("ep"), lax.axis_size("tp"))
    path = fused_shards if grid == (LINE * BLOCKS, PLANES * CORES) else routed_shards
    return path(tokens, cotangent, routes, router, w_gate, w_up, w_down)


def solution(mesh):
    placed = (
        P("ep", None),
        P("ep", None),
        P("ep", None),
        P(),
        P("ep", None, "tp"),
        P("ep", None, "tp"),
        P("ep", "tp", None),
    )
    return jax.shard_map(
        shards,
        mesh=mesh,
        in_specs=placed,
        out_specs=(
            P("ep", "tp"),
            P("ep", None),
            P("ep", None, "tp"),
            P("ep", None, "tp"),
            P("ep", "tp", None),
            P(("ep", "tp"), None),
        ),
        check_vma=False,
    )
```

```python
import jax
import jax.numpy as jnp
from jax import lax
from jax.experimental import pallas as pl
from jax.experimental.pallas import tpu as pltpu
from jax.sharding import PartitionSpec as P

BLOCKS = 2
CORES = 2
PLANES = 2
LINE = 4
PIECES = 1
SIXTEENTHS = 9
VMEM_LIMIT = 40 * 1024 * 1024
MESH = pl.DeviceIdType.MESH


def build_slots(block_routes, experts, capacity):
    flat_routes = block_routes.reshape(-1)
    labels = jnp.arange(experts, dtype=jnp.int32)
    hit_mask = (flat_routes[None, :] == labels[:, None]).astype(jnp.int32)
    rank_in = jnp.cumsum(hit_mask, axis=1, dtype=jnp.int32) - 1
    slot_ids = jnp.arange(capacity, dtype=jnp.int32)
    assigned = (hit_mask[:, None, :] == 1) & (rank_in[:, None, :] == slot_ids[None, :, None])
    return assigned.astype(jnp.float32)


def gate_pair(tokens, routes, router, experts):
    logits = jnp.dot(tokens, router, preferred_element_type=jnp.float32)
    labels = jnp.arange(experts, dtype=jnp.int32)
    picked = (routes[:, :, None] == labels[None, None, :]).astype(jnp.float32)
    chosen = jnp.sum(picked * logits[:, None, :], axis=2)
    margin = chosen[:, 0] - chosen[:, 1]
    weights = jnp.stack([jax.nn.sigmoid(margin), jax.nn.sigmoid(-margin)], axis=1)
    return (picked, weights)


def logit_grads(picked, weights, gate_grad):
    lead_grad = weights[:, 0] * weights[:, 1] * (gate_grad[:, 0] - gate_grad[:, 1])
    pair_grad = jnp.stack([lead_grad, -lead_grad], axis=1)
    return jnp.sum(picked * pair_grad[:, :, None], axis=1)


def expert_grads(rows_in, cot_in, gate_in, gate_weight, up_weight, down_weight):
    pre_gate = jnp.dot(rows_in, gate_weight, preferred_element_type=jnp.float32)
    pre_up = jnp.dot(rows_in, up_weight, preferred_element_type=jnp.float32)
    back_grad = lax.dot_general(
        cot_in, down_weight, (((1,), (1,)), ((), ())), preferred_element_type=jnp.float32
    )
    sig_gate = jax.nn.sigmoid(pre_gate)
    active = pre_gate * sig_gate
    hidden = (active * pre_up).astype(jnp.bfloat16)
    gate_terms = jnp.sum(hidden.astype(jnp.float32) * back_grad, axis=1)
    gate_col = gate_in.astype(jnp.float32)[:, None]
    scaled_back = gate_col * back_grad
    d_gate = (scaled_back * pre_up * sig_gate * (1.0 + pre_gate * (1.0 - sig_gate))).astype(
        jnp.bfloat16
    )
    d_up = (scaled_back * active).astype(jnp.bfloat16)
    scaled_cot = (gate_col * cot_in.astype(jnp.float32)).astype(jnp.bfloat16)
    contract_rows = (((0,), (0,)), ((), ()))
    grad_gate = lax.dot_general(
        rows_in, d_gate, contract_rows, preferred_element_type=jnp.float32
    ).astype(jnp.bfloat16)
    grad_up = lax.dot_general(
        rows_in, d_up, contract_rows, preferred_element_type=jnp.float32
    ).astype(jnp.bfloat16)
    grad_down = lax.dot_general(
        hidden, scaled_cot, contract_rows, preferred_element_type=jnp.float32
    ).astype(jnp.bfloat16)
    return (d_gate, d_up, gate_terms, grad_gate, grad_up, grad_down)


def spread_slabs(packed, experts, slab_count):
    widened = jnp.broadcast_to(packed[:, None], (experts, BLOCKS) + packed.shape[1:])
    return widened.reshape((slab_count,) + packed.shape[1:])


def routed_shards(tokens, cotangent, routes, router, w_gate, w_up, w_down):
    highest = lax.Precision.HIGHEST
    ep_count = lax.axis_size("ep")
    tp_count = lax.axis_size("tp")
    experts = ep_count // BLOCKS
    tok_rows, width = tokens.shape
    top_count = routes.shape[1]
    capacity = 3 * tok_rows * top_count // (2 * experts)
    col_width = width // tp_count
    tp_index = lax.axis_index("tp")
    picked, weights = gate_pair(tokens, routes, router, experts)
    assigned = build_slots(routes, experts, capacity)
    per_token = jnp.sum(assigned.reshape(experts, capacity, tok_rows, top_count), axis=3)
    token_map = per_token.astype(jnp.bfloat16)
    gate_send = weights.astype(jnp.bfloat16)
    gate_slots = jnp.einsum(
        "ecj,j->ec", assigned, gate_send.astype(jnp.float32).reshape(-1), precision=highest
    ).astype(jnp.bfloat16)
    gate_out = spread_slabs(gate_slots, experts, ep_count)

    def pack_rows(source):
        packed = jnp.einsum(
            "ect,td->ecd", token_map, source, preferred_element_type=jnp.float32
        ).astype(jnp.bfloat16)
        return spread_slabs(packed, experts, ep_count)

    tok_part = lax.dynamic_slice_in_dim(tokens, tp_index * col_width, col_width, 1)
    cot_part = lax.dynamic_slice_in_dim(cotangent, tp_index * col_width, col_width, 1)
    recv_part, recv_cot_part, recv_gate = (
        lax.all_to_all(pack_rows(tok_part), "ep", split_axis=0, concat_axis=0, tiled=True),
        lax.all_to_all(pack_rows(cot_part), "ep", split_axis=0, concat_axis=0, tiled=True),
        lax.all_to_all(gate_out, "ep", split_axis=0, concat_axis=0, tiled=True),
    )
    recv_rows, recv_cot = (
        lax.all_gather(recv_part, "tp", axis=2, tiled=True),
        lax.all_gather(recv_cot_part, "tp", axis=2, tiled=True),
    )
    rows_in = recv_rows.reshape(-1, width)
    cot_in = recv_cot.reshape(-1, width)
    gate_in = recv_gate.reshape(-1)
    d_gate, d_up, gate_terms, grad_gate, grad_up, grad_down = expert_grads(
        rows_in, cot_in, gate_in, w_gate[0], w_up[0], w_down[0]
    )
    contract_hidden = (((1,), (1,)), ((), ()))
    partial_dx = lax.dot_general(
        d_gate, w_gate[0], contract_hidden, preferred_element_type=jnp.float32
    )
    partial_dx = partial_dx + lax.dot_general(
        d_up, w_up[0], contract_hidden, preferred_element_type=jnp.float32
    )
    summed_dx = lax.psum_scatter(
        partial_dx.reshape(ep_count, capacity, width).astype(jnp.bfloat16),
        "tp",
        scatter_dimension=2,
        tiled=True,
    ).astype(jnp.float32)
    gate_sums = lax.psum(gate_terms.reshape(ep_count, capacity), "tp")
    back_dx, back_gate = (
        lax.all_to_all(
            summed_dx.astype(jnp.bfloat16), "ep", split_axis=0, concat_axis=0, tiled=True
        ).astype(summed_dx.dtype),
        lax.all_to_all(
            gate_sums.astype(jnp.bfloat16), "ep", split_axis=0, concat_axis=0, tiled=True
        ).astype(gate_sums.dtype),
    )
    slab_dx = jnp.sum(back_dx.reshape(experts, BLOCKS, capacity, col_width), axis=1)
    routed_dx = jnp.einsum("ect,ecd->td", per_token, slab_dx, precision=highest)
    slab_gate = jnp.sum(back_gate.reshape(experts, BLOCKS, capacity), axis=1)
    gate_grad = jnp.einsum("ecj,ec->j", assigned, slab_gate, precision=highest).reshape(
        tok_rows, top_count
    )
    logit_grad = logit_grads(picked, weights, gate_grad)
    router_cols = lax.dynamic_slice_in_dim(router, tp_index * col_width, col_width, 0).astype(
        jnp.float32
    )
    token_grad = (routed_dx + jnp.dot(logit_grad, router_cols.T, precision=highest)).astype(
        jnp.bfloat16
    )
    seg_rows = tok_rows // tp_count
    own_rows = lax.dynamic_slice_in_dim(tokens, tp_index * seg_rows, seg_rows, 0).astype(
        jnp.float32
    )
    own_logit = lax.dynamic_slice_in_dim(logit_grad, tp_index * seg_rows, seg_rows, 0)
    router_grad = lax.psum_scatter(
        jnp.dot(own_rows.T, own_logit, precision=highest),
        ("ep", "tp"),
        scatter_dimension=0,
        tiled=True,
    )
    return (token_grad, gate_grad, grad_gate[None], grad_up[None], grad_down[None], router_grad)


class Place:
    def __init__(self):
        ep, self.tp = lax.axis_index("ep"), lax.axis_index("tp")
        self.z, self.x = ep // BLOCKS, ep % BLOCKS
        self.y, self.c = self.tp // CORES, self.tp % CORES
        self.pair = self.z + 1 - 2 * (self.z % 2)
        self.near = 2 - self.z // 2
        self.far = 3 * (1 - self.z // 2)
        self.rank = 3 - (self.z + 1) // 2 % 2
        self.lines = (self.pair, self.near, self.far)
        self.slots = (1, self.rank, self.rank)

    def device(self, z, x):
        return {"ep": z * BLOCKS + x, "tp": self.tp}

    def along(self, z):
        return self.device(z, self.x)

    def across(self):
        return self.device(self.z, 1 - self.x)

    def other_plane(self):
        return {"ep": self.z * BLOCKS + self.x, "tp": (1 - self.y) * CORES + self.c}

    def other_core(self):
        return {"ep": self.z * BLOCKS + self.x, "tp": self.y * CORES + 1 - self.c}

    def diagonal(self):
        return {"ep": self.z * BLOCKS + 1 - self.x, "tp": (1 - self.y) * CORES + self.c}

    def announce(self):
        peers = [self.along(z) for z in self.lines]
        peers += [self.across(), self.other_plane(), self.diagonal(), self.other_core()]
        for peer in peers:
            pl.semaphore_signal(
                pltpu.get_barrier_semaphore(), inc=1, device_id=peer, device_id_type=MESH
            )
        return len(peers)


SCHEDULE = (
    "X00", "Z10", "X10", "Y010", "Z20", "F0", "D0", "X20", "Y110", "Y100", "Z30", "Y200", "F1",
    "Y210", "D1", "X30", "F2", "D2", "A1", "Y300", "A2", "Y310", "F3", "D3", "G0", "G1", "A3",
    "W0", "E1", "W1", "E2", "R0", "W2", "G2", "R1", "A0", "E3", "G3", "R2", "E0", "T", "R3",
)


def fused_kernel(
    tok_hbm, cot_hbm, routes_hbm, router_hbm, wg_hbm, wu_hbm, wd_hbm,
    tg_ref, gg_ref, gw_ref, gu_ref, gd_ref, rg_ref,
    src, wgu, wd, rows, pack, hot, gate_send, gate_recv, gate_col,
    routes_ref, router_ref, router_all, hs, dgu, dx_send, dx_own, c_recv, s_send, s_recv, s_own, z_send, z_recv,
    g_sum, g_send, g_recv, gz_recv, coefs, term_col, r_send, r_core, r_sum, r_recv, rz_send, rz_recv,
    load_sems, z_sems, x_sems, y_sems, c_sems, gz_sems, gx_sems,
    sc_sems, s_sems, sz_sems, gp_sems, gl_sems, r_sems,
):
    f32, bf16 = jnp.float32, jnp.bfloat16
    at = Place()
    cap, tok_rows, width = pack.shape[1], src.shape[1], src.shape[2]
    hidden, part = wd.shape[0], tg_ref.shape[1]
    span = pack.shape[2]
    rest = width - span
    size = cap // PIECES
    window = pl.ds(pl.multiple_of(at.y * rest, 128), span)
    outer = pl.ds(pl.multiple_of(at.y * span, 128), rest)
    inner = pl.ds(pl.multiple_of((1 - at.y) * span, 128), rest)
    started = []

    def dot(lhs, rhs, dims):
        return lax.dot_general(lhs, rhs, (dims, ((), ())), preferred_element_type=f32)

    def send(source, target, send_sem, recv_sem, peer):
        copy = pltpu.make_async_remote_copy(
            src_ref=source, dst_ref=target, send_sem=send_sem, recv_sem=recv_sem,
            device_id=peer, device_id_type=MESH,
        )
        copy.start()
        started.append(copy)

    def arrived(target, sem):
        pltpu.make_async_remote_copy(
            src_ref=target, dst_ref=target, send_sem=sem, recv_sem=sem,
            device_id=at.across(), device_id_type=MESH,
        ).wait_recv()

    greeted = at.announce()
    def thirds(value):
        high = value.astype(bf16).astype(f32)
        middle = (value - high).astype(bf16).astype(f32)
        return [high, middle, (value - high - middle).astype(bf16).astype(f32)]

    loads = [
        pltpu.make_async_copy(routes_hbm, routes_ref, load_sems.at[5]),
        pltpu.make_async_copy(tok_hbm, src.at[0], load_sems.at[0]),
        pltpu.make_async_copy(cot_hbm, src.at[1], load_sems.at[1]),
        pltpu.make_async_copy(router_hbm, router_ref, load_sems.at[6]),
        pltpu.make_async_copy(wg_hbm, wgu.at[:, pl.ds(0, hidden)], load_sems.at[2]),
        pltpu.make_async_copy(wu_hbm, wgu.at[:, pl.ds(hidden, hidden)], load_sems.at[3]),
        pltpu.make_async_copy(wd_hbm, wd, load_sems.at[4]),
    ]
    for copy in loads:
        copy.start()
    loads[0].wait()

    side = hot.shape[1]
    row8 = lax.broadcasted_iota(jnp.int32, (8, tok_rows), 0)
    first, second = routes_ref[0:1, :], routes_ref[1:2, :]
    is_first, is_second = first == row8, second == row8
    hit = jnp.where(is_first | is_second, 1.0, 0.0)
    up_to = lax.broadcasted_iota(jnp.int32, (tok_rows, tok_rows), 0) <= lax.broadcasted_iota(
        jnp.int32, (tok_rows, tok_rows), 1
    )
    place = dot(hit, jnp.where(up_to, 1.0, 0.0), ((1,), (0,)))
    place = jnp.where(hit > 0.0, place, 0.0)
    slot = (lax.broadcasted_iota(jnp.int32, (side, tok_rows), 0) + 1).astype(f32)
    for e in range(LINE):
        hot[e] = jnp.where(slot == place[e : e + 1, :], 1.0, 0.0).astype(bf16)
    loads[1].wait()
    loads[2].wait()

    def piece(k, j, h):
        return pl.ds((k * BLOCKS + j) * cap + h * size, size)

    def chunk(k):
        return slice(k * BLOCKS * cap, (k + 1) * BLOCKS * cap)

    def pass_x(k, h):
        send(
            rows.at[at.c, piece(k, 0, h), window], rows.at[at.c, piece(k, 1, h), window],
            x_sems.at[0, k, h], x_sems.at[1, k, h], at.across(),
        )

    def pass_y(k, j, h):
        ref = rows.at[at.c, piece(k, j, h), outer]
        send(ref, ref, y_sems.at[0, k, j, h], y_sems.at[1, k, j, h], at.other_plane())

    def pass_c(k, j, h):
        ref = rows.at[at.c, piece(k, j, h), :]
        send(ref, ref, c_sems.at[0, k, j, h], c_sems.at[1, k, j, h], at.other_core())

    own_hot = hot[at.z, 0:cap, :]
    rows[at.c, 0:cap, :] = dot(own_hot, src[at.c], ((1,), (0,))).astype(bf16)
    for m in range(LINE - 1):
        pack[m] = dot(
            hot[at.lines[m], 0:cap, :], src[at.c, :, window], ((1,), (0,))
        ).astype(bf16)
    pl.semaphore_wait(pltpu.get_barrier_semaphore(), greeted)
    for h in range(PIECES):
        pass_x(0, h)
    order = [(m, h) for m in range(LINE - 1) for h in range(PIECES)]
    for m, h in order:
        begin = pl.multiple_of(at.slots[m] * BLOCKS * cap + h * size, 16)
        send(
            pack.at[m, pl.ds(h * size, size), :], rows.at[at.c, pl.ds(begin, size), window],
            z_sems.at[0, m, h], z_sems.at[1, at.slots[m], h], at.along(at.lines[m]),
        )

    experts = router_ref.shape[0]
    loads[3].wait()
    router_all[0:experts, :] = router_ref[...].astype(f32)
    router_all[experts:, :] = jnp.zeros((8 - experts, width), f32)
    logits = dot(router_all[...].astype(bf16), src[0], ((1,), (1,)))
    chosen = [
        jnp.sum(jnp.where(mask, logits, 0.0), axis=0, keepdims=True)
        for mask in (is_first, is_second)
    ]
    margin = chosen[0] - chosen[1]
    weights = [jax.nn.sigmoid(margin), jax.nn.sigmoid(-margin)]
    sent = [w.astype(bf16).astype(f32) for w in weights]
    by_expert = jnp.where(is_first, sent[0], 0.0) + jnp.where(is_second, sent[1], 0.0)
    notes = [(first + second).astype(f32)] + thirds(weights[0] * weights[1])
    for n, note in enumerate(notes):
        by_expert = jnp.where(row8 == LINE + n, note, by_expert)
    for m, z in enumerate((at.z,) + at.lines):
        gate_send[m] = dot(by_expert.astype(bf16), hot[z], ((1,), (1,)))
    gate_recv[0] = gate_send[0]
    send(gate_send.at[0], gate_recv.at[1], gx_sems.at[0, 0], gx_sems.at[1, 0], at.across())
    for m in range(LINE - 1):
        send(
            gate_send.at[m + 1], gate_recv.at[at.slots[m] * BLOCKS],
            gz_sems.at[0, m], gz_sems.at[1, at.slots[m]], at.along(at.lines[m]),
        )
    rows[1 - at.c, 0:cap, :] = dot(own_hot, src[1 - at.c], ((1,), (0,))).astype(bf16)
    g_sum[...] = jnp.zeros_like(g_sum)

    row_id = lax.broadcasted_iota(jnp.int32, (side, side), 0)
    lane_id = lax.broadcasted_iota(jnp.int32, (side, side), 1)
    top8 = lax.broadcasted_iota(jnp.int32, (8, side), 0)
    diagonal = row_id == lane_id

    def to_column(row):
        return jnp.sum(jnp.where(diagonal, row, 0.0), axis=1, keepdims=True)

    def take_row(tile, index):
        return jnp.sum(jnp.where(top8 == index, tile, 0.0), axis=0, keepdims=True)

    sources = (at.z,) + at.lines

    def step_z(k, h):
        arrived(rows.at[at.c, piece(k, 0, h), window], z_sems.at[1, k, h])
        pass_x(k, h)
        pass_y(k, 0, h)
        if h == 0:
            arrived(gate_recv.at[k * BLOCKS], gz_sems.at[1, k])
            send(
                gate_recv.at[k * BLOCKS], gate_recv.at[k * BLOCKS + 1],
                gx_sems.at[0, k], gx_sems.at[1, k], at.across(),
            )

    def step_x(k, h):
        arrived(rows.at[at.c, piece(k, 1, h), window], x_sems.at[1, k, h])
        pass_y(k, 1, h)

    def step_y(k, j, h):
        arrived(rows.at[at.c, piece(k, j, h), inner], y_sems.at[1, k, j, h])
        pass_c(k, j, h)

    def forward(k):
        arrived(gate_recv.at[k * BLOCKS + 1], gx_sems.at[1, k])
        for j in range(BLOCKS):
            column = to_column(take_row(gate_recv[k * BLOCKS + j], at.z))
            base = (k * BLOCKS + j) * cap
            gate_col[base : base + cap, :] = jnp.broadcast_to(column[0:cap], (cap, side))
        for j in range(BLOCKS):
            if (k, j) != (0, 0):
                for h in range(PIECES):
                    arrived(rows.at[1 - at.c, piece(k, j, h), :], c_sems.at[1, k, j, h])
        if k == 0:
            for copy in loads[4:]:
                copy.wait()
        both = dot(rows[0, chunk(k), :], wgu[...], ((1,), (0,)))
        pre_gate, pre_up = both[:, :hidden], both[:, hidden:]
        back = dot(rows[1, chunk(k), :], wd[...], ((1,), (1,)))
        gate = gate_col[chunk(k), 0:1]
        sig = jax.nn.sigmoid(pre_gate)
        active = pre_gate * sig
        product = active * pre_up
        terms = jnp.sum(product.astype(bf16).astype(f32) * back, axis=1, keepdims=True)
        scaled = gate * back
        dgu[chunk(k), 0:hidden] = (scaled * pre_up * sig * (1.0 + pre_gate * (1.0 - sig))).astype(bf16)
        dgu[chunk(k), hidden:] = (scaled * active).astype(bf16)
        hs[chunk(k), :] = (gate * product).astype(bf16)
        term_col[chunk(k), :] = jnp.broadcast_to(terms, (BLOCKS * cap, side))
        for j in range(BLOCKS):
            line = jnp.sum(
                jnp.where(diagonal[0:cap], terms[j * cap : (j + 1) * cap], 0.0),
                axis=0, keepdims=True,
            )
            block = sources[k] * BLOCKS + (at.x if j == 0 else 1 - at.x)
            g_sum[...] += jnp.where(top8 == block, line, 0.0)

    def input_grad(k, plane, core):
        begin = pl.multiple_of((plane * CORES + core) * part, part)
        return dot(dgu[chunk(k), :], wgu[pl.ds(begin, part), :], ((1,), (1,)))

    def backward(k):
        for p in range(PLANES):
            dx_send[k, p] = input_grad(k, p, 1 - at.c).astype(bf16)
            send(
                dx_send.at[k, p], c_recv.at[k, p],
                sc_sems.at[0, k, p], sc_sems.at[1, k, p], at.other_core(),
            )
        for n, plane in enumerate((1 - at.y, at.y)):
            dx_own[k, n] = input_grad(k, plane, at.c)

    def after_c(k):
        for p in range(PLANES):
            arrived(c_recv.at[k, p], sc_sems.at[1, k, p])

        def summed(n, plane, j):
            part_rows = slice(j * cap, (j + 1) * cap)
            return dx_own[k, n, part_rows, :] + c_recv[k, plane, part_rows, :].astype(f32)

        ways = (
            (0, 1 - at.y, 1, at.diagonal), (1, at.y, 1, at.across), (0, 1 - at.y, 0, at.other_plane),
        )
        for i, (n, plane, j, peer) in enumerate(ways):
            s_send[k, i] = summed(n, plane, j).astype(bf16)
            send(
                s_send.at[k, i], s_recv.at[k, i], s_sems.at[0, k, i], s_sems.at[1, k, i], peer()
            )
        s_own[k] = summed(1, at.y, 0)

    def after_x(k):
        total = s_own[k]
        for i in range(3):
            arrived(s_recv.at[k, i], s_sems.at[1, k, i])
            total = total + s_recv[k, i].astype(f32)
        total = total.astype(bf16)
        if k == 0:
            z_recv[at.z] = total
            return
        z_send[k - 1] = total
        mine = 1 if k == 1 else at.rank
        send(
            z_send.at[k - 1], z_recv.at[at.z],
            sz_sems.at[0, k], sz_sems.at[1, mine], at.along(sources[k]),
        )

    def gate_stage(n):
        if n == 0:
            send(g_sum, g_recv.at[0], gp_sems.at[0, 0], gp_sems.at[1, 0], at.other_core())
        elif n == 1:
            arrived(g_recv.at[0], gp_sems.at[1, 0])
            g_send[0] = g_sum[...] + g_recv[0]
            for i, peer in enumerate((at.across, at.other_plane, at.diagonal), 1):
                send(g_send.at[0], g_recv.at[i], gp_sems.at[0, i], gp_sems.at[1, i], peer())
        elif n == 2:
            total = g_send[0]
            for i in range(1, 4):
                arrived(g_recv.at[i], gp_sems.at[1, i])
                total = total + g_recv[i]
            g_send[1] = total
            gz_recv[at.z] = total
            for m in range(LINE - 1):
                send(
                    g_send.at[1], gz_recv.at[at.z],
                    gl_sems.at[0, m], gl_sems.at[1, at.slots[m]], at.along(at.lines[m]),
                )
        else:
            gate_finish()

    state = {}

    def split3(value):
        return jnp.concatenate(thirds(value) + [jnp.zeros_like(value)], axis=0).astype(bf16)

    def gate_finish():
        for m in range(LINE - 1):
            arrived(gz_recv.at[at.lines[m]], gl_sems.at[1, m + 1])
        own = at.z * BLOCKS + at.x
        grads = [jnp.zeros((1, tok_rows), f32)] * 2
        for e in range(LINE):
            column = to_column(take_row(gz_recv[e], own))
            term = jnp.sum(column * hot[e].astype(f32), axis=0, keepdims=True)
            grads[0] = grads[0] + jnp.where(first == e, term, 0.0)
            grads[1] = grads[1] + jnp.where(second == e, term, 0.0)
        gg_ref[...] = jnp.where(row8 == 0, grads[0], jnp.where(row8 == 1, grads[1], 0.0))
        lead = weights[0] * weights[1] * (grads[0] - grads[1])
        logit_grad = jnp.where(is_first, lead, 0.0) - jnp.where(is_second, lead, 0.0)
        state["parts"] = split3(logit_grad)

    def token_finish():
        begin = pl.multiple_of(at.tp * part, part)
        columns = router_all[:, pl.ds(begin, part)]
        triple = jnp.concatenate([columns] * 3 + [jnp.zeros_like(columns)], axis=0).astype(bf16)
        total = dot(state["parts"], triple, ((0,), (0,)))
        for m in range(LINE - 1):
            arrived(z_recv.at[at.lines[m]], sz_sems.at[1, m + 1])
        for e in range(LINE):
            total = total + dot(hot[e, 0:cap, :], z_recv[e], ((0,), (0,)))
        tg_ref[...] = total.astype(bf16)

    def router_stage(n):
        if n == 0:
            lanes = lax.broadcasted_iota(jnp.int32, (cap, side), 1)
            expert = lanes % 8
            for b in range(LINE * BLOCKS):
                notes = gate_recv[b]
                other = to_column(notes[4:5])[0:cap].astype(jnp.int32) - at.z
                lead = to_column(notes[5:6] + notes[6:7] + notes[7:8])[0:cap]
                lead = lead * term_col[b * cap : (b + 1) * cap, :]
                lead = jnp.where(expert == at.z, lead, jnp.where(expert == other, -lead, 0.0))
                high, middle, low = thirds(lead)
                coefs[b * cap : (b + 1) * cap, :] = jnp.where(
                    lanes < 8, high, jnp.where(lanes < 16, middle, jnp.where(lanes < 24, low, 0.0))
                ).astype(bf16)
            sums = dot(coefs[...], rows[0], ((0,), (0,)))
            sums = sums[0:8] + sums[8:16] + sums[16:24]
            wide = r_send.shape[3]
            for z in range(LINE):
                for x in range(BLOCKS):
                    begin = (z * BLOCKS + x) * wide
                    r_send[x, z] = sums[:, begin : begin + wide]
            send(r_send, r_core, r_sems.at[0, 0], r_sems.at[1, 0], at.other_core())
            return
        if n == 1:
            arrived(r_core, r_sems.at[1, 0])
            r_sum[...] = r_send[...] + r_core[...]
            ways = ((1 - at.x, at.across), (at.x, at.other_plane), (1 - at.x, at.diagonal))
            for i, (x, peer) in enumerate(ways):
                send(
                    r_sum.at[x], r_recv.at[i], r_sems.at[0, 1 + i], r_sems.at[1, 1 + i], peer()
                )
            return
        if n == 2:
            total = r_sum[at.x]
            for i in range(3):
                arrived(r_recv.at[i], r_sems.at[1, 1 + i])
                total = total + r_recv[i]
            rz_send[...] = total
            for m in range(LINE - 1):
                send(
                    rz_send.at[at.lines[m]], rz_recv.at[at.slots[m] - 1],
                    r_sems.at[0, m + 4], r_sems.at[1, at.slots[m] + 3], at.along(at.lines[m]),
                )
            return
        total = rz_send[at.z]
        for m in range(LINE - 1):
            arrived(rz_recv.at[m], r_sems.at[1, m + 4])
            total = total + rz_recv[m]
        seg = rg_ref.shape[1]
        own = jnp.zeros((8, seg), f32)
        for i in range(PLANES * CORES):
            own = jnp.where(at.tp == i, total[:, i * seg : (i + 1) * seg], own)
        rg_ref[...] = own

    tile = 256

    def weight_grads(n):
        if n < 2:
            half = width // tile // 2
            for m in range(n * half, (n + 1) * half):
                columns = slice(m * tile, (m + 1) * tile)
                both = dot(rows[0, :, columns], dgu[...], ((0,), (0,))).astype(bf16)
                gw_ref[columns, :] = both[:, :hidden]
                gu_ref[columns, :] = both[:, hidden:]
            return
        for m in range(hidden // tile):
            columns = slice(m * tile, (m + 1) * tile)
            gd_ref[columns, :] = dot(hs[:, columns], rows[1], ((0,), (0,))).astype(bf16)

    steps = {
        "X": step_x, "Z": step_z, "Y": step_y, "F": forward, "D": backward, "A": after_c,
        "E": after_x, "G": gate_stage, "W": weight_grads, "T": token_finish, "R": router_stage,
    }
    for token in SCHEDULE:
        steps[token[0]](*[int(digit) for digit in token[1:]])
    for copy in started:
        copy.wait_send()


def store_kernel(tg_in, gg_in, gw_in, gu_in, gd_in, rg_in, tg, gg, gw, gu, gd, rg, gates, router, sems):
    gates[...] = gg_in[0 : gates.shape[0], :]
    router[...] = rg_in[0 : router.shape[0], :]
    copies = []
    for source, target in ((gw_in, gw), (gu_in, gu), (gd_in, gd), (tg_in, tg), (gates, gg), (router, rg)):
        copies.append(pltpu.make_async_copy(source, target, sems.at[len(copies)]))
        copies[-1].start()
    for copy in copies:
        copy.wait()


def in_hbm(array):
    return pltpu.with_memory_space_constraint(array, pltpu.HBM)


def fused_shards(tokens, cotangent, routes, router, w_gate, w_up, w_down):
    ep_count, tp_count = lax.axis_size("ep"), lax.axis_size("tp")
    experts = ep_count // BLOCKS
    tok_rows, width = tokens.shape
    cap = 3 * tok_rows * routes.shape[1] // (2 * experts)
    part, hidden = width // tp_count, w_down.shape[1]
    span = SIXTEENTHS * width // 16
    seg, wide = width // (ep_count * tp_count), width // ep_count
    dma = pltpu.SemaphoreType.DMA
    bf16, f32 = jnp.bfloat16, jnp.float32
    vmem = pl.BlockSpec(memory_space=pltpu.VMEM)
    hbm = pl.BlockSpec(memory_space=pltpu.HBM)
    total, pair = ep_count * cap, BLOCKS * cap
    tiny = (8, 128)
    results = pl.pallas_call(
        fused_kernel,
        out_shape=(
            jax.ShapeDtypeStruct((tok_rows, part), bf16),
            jax.ShapeDtypeStruct((8, tok_rows), f32),
            jax.ShapeDtypeStruct((width, hidden), bf16),
            jax.ShapeDtypeStruct((width, hidden), bf16),
            jax.ShapeDtypeStruct((hidden, width), bf16),
            jax.ShapeDtypeStruct((8, seg), f32),
        ),
        in_specs=[hbm] * 7,
        out_specs=[vmem] * 6,
        scratch_shapes=[
            pltpu.VMEM((2, tok_rows, width), bf16),
            pltpu.VMEM((width, 2 * hidden), bf16),
            pltpu.VMEM((hidden, width), bf16),
            pltpu.VMEM((2, total, width), bf16),
            pltpu.VMEM((LINE - 1, cap, span), bf16),
            pltpu.VMEM((LINE, 128, tok_rows), bf16),
            pltpu.VMEM((LINE,) + tiny, f32),
            pltpu.VMEM((ep_count,) + tiny, f32),
            pltpu.VMEM((total, 128), f32),
            pltpu.VMEM((routes.shape[1], tok_rows), jnp.int32),
            pltpu.VMEM((experts, width), bf16),
            pltpu.VMEM((8, width), f32),
            pltpu.VMEM((total, hidden), bf16),
            pltpu.VMEM((total, 2 * hidden), bf16),
            pltpu.VMEM((LINE, PLANES, pair, part), bf16),
            pltpu.VMEM((LINE, PLANES, pair, part), f32),
            pltpu.VMEM((LINE, PLANES, pair, part), bf16),
            pltpu.VMEM((LINE, 3, cap, part), bf16),
            pltpu.VMEM((LINE, 3, cap, part), bf16),
            pltpu.VMEM((LINE, cap, part), f32),
            pltpu.VMEM((LINE - 1, cap, part), bf16),
            pltpu.VMEM((LINE, cap, part), bf16),
            pltpu.VMEM(tiny, f32),
            pltpu.VMEM((2,) + tiny, f32),
            pltpu.VMEM((4,) + tiny, f32),
            pltpu.VMEM((LINE,) + tiny, f32),
            pltpu.VMEM((total, 128), bf16),
            pltpu.VMEM((total, 128), f32),
            pltpu.VMEM((BLOCKS, LINE, 8, wide), f32),
            pltpu.VMEM((BLOCKS, LINE, 8, wide), f32),
            pltpu.VMEM((BLOCKS, LINE, 8, wide), f32),
            pltpu.VMEM((3, LINE, 8, wide), f32),
            pltpu.VMEM((LINE, 8, wide), f32),
            pltpu.VMEM((LINE - 1, 8, wide), f32),
            dma((7,)),
            dma((2, LINE, PIECES)),
            dma((2, LINE, PIECES)),
            dma((2, LINE, BLOCKS, PIECES)),
            dma((2, LINE, BLOCKS, PIECES)),
            dma((2, LINE)),
            dma((2, LINE)),
            dma((2, LINE, PLANES)),
            dma((2, LINE, 3)),
            dma((2, LINE)),
            dma((2, 4)),
            dma((2, LINE)),
            dma((2, 7)),
        ],
        compiler_params=pltpu.CompilerParams(
            collective_id=0, has_side_effects=True, vmem_limit_bytes=VMEM_LIMIT
        ),
    )(*map(in_hbm, (tokens, cotangent, routes.T, router.T, w_gate[0], w_up[0], w_down[0])))
    top = routes.shape[1]
    token_grad, gates, grad_gate, grad_up, grad_down, router_grad = pl.pallas_call(
        store_kernel,
        out_shape=(
            jax.ShapeDtypeStruct((tok_rows, part), bf16),
            jax.ShapeDtypeStruct((top, tok_rows), f32),
            jax.ShapeDtypeStruct((width, hidden), bf16),
            jax.ShapeDtypeStruct((width, hidden), bf16),
            jax.ShapeDtypeStruct((hidden, width), bf16),
            jax.ShapeDtypeStruct((experts, seg), f32),
        ),
        in_specs=[vmem] * 6,
        out_specs=[hbm] * 6,
        scratch_shapes=[
            pltpu.VMEM((top, tok_rows), f32),
            pltpu.VMEM((experts, seg), f32),
            dma((6,)),
        ],
        compiler_params=pltpu.CompilerParams(vmem_limit_bytes=16 * 1024 * 1024),
    )(*results)
    return (
        token_grad,
        gates.T,
        grad_gate[None],
        grad_up[None],
        grad_down[None],
        router_grad.T,
    )


def shards(tokens, cotangent, routes, router, w_gate, w_up, w_down):
    grid = (lax.axis_size("ep"), lax.axis_size("tp"))
    path = fused_shards if grid == (LINE * BLOCKS, PLANES * CORES) else routed_shards
    return path(tokens, cotangent, routes, router, w_gate, w_up, w_down)


def solution(mesh):
    placed = (
        P("ep", None),
        P("ep", None),
        P("ep", None),
        P(),
        P("ep", None, "tp"),
        P("ep", None, "tp"),
        P("ep", "tp", None),
    )
    return jax.shard_map(
        shards,
        mesh=mesh,
        in_specs=placed,
        out_specs=(
            P("ep", "tp"),
            P("ep", None),
            P("ep", None, "tp"),
            P("ep", None, "tp"),
            P("ep", "tp", None),
            P(("ep", "tp"), None),
        ),
        check_vma=False,
    )
```
